32 devices in a mesh: ep: 16 (over z, y, x), tp: 2 (over core).
Axes of the slice: x: 2, y: 2, z: 4, core: 2. Of those that a mesh axis runs over, the one named last changes fastest.
Arguments:
- hidden: bfloat16 [1024, 2048], P('ep'), may hold values from -6 to 6
- mix_gain: float32 [2048], replicated, may hold values from 0.1 to 1.9
- recept_weight: bfloat16 [2048, 1024], P(None, 'tp'), may hold values from -0.125 to 0.125
- key_weight: bfloat16 [2048, 1024], P(None, 'tp'), may hold values from -0.125 to 0.125
- value_weight: bfloat16 [2048, 1024], P(None, 'tp'), may hold values from -0.125 to 0.125
- decay_down: bfloat16 [2048, 64], replicated, may hold values from -0.125 to 0.125
- decay_up: bfloat16 [64, 1024], replicated, may hold values from -0.75 to 0.75
- decay_bias: float32 [1024], replicated, may hold values from -4 to 1
- rate_down: bfloat16 [2048, 64], replicated, may hold values from -0.125 to 0.125
- rate_up: bfloat16 [64, 1024], replicated, may hold values from -0.75 to 0.75
- rate_bias: float32 [1024], replicated, may hold values from -4 to 4
- head_gain: float32 [1024], replicated, may hold values from 0.1 to 1.9
- out_weight: bfloat16 [1024, 2048], P('tp'), may hold values from -0.1875 to 0.1875
- memory_state: float32 [1024, 16, 64, 64], P('ep', 'tp'), may hold values from -6 to 6
- ffn_gain: float32 [2048], replicated, may hold values from 0.1 to 1.9
- blend_vector: bfloat16 [2048], replicated, may hold values from -0.125 to 0.125
- dense_gate: bfloat16 [2048, 5632], P(None, ('ep', 'tp')), may hold values from -0.125 to 0.125
- dense_up: bfloat16 [2048, 5632], P(None, ('ep', 'tp')), may hold values from -0.125 to 0.125
- dense_down: bfloat16 [5632, 2048], P(('ep', 'tp')), may hold values from -0.3125 to 0.3125
- expert_gate: bfloat16 [16, 2048, 1536], P('ep', None, 'tp'), may hold values from -0.125 to 0.125
- expert_up: bfloat16 [16, 2048, 1536], P('ep', None, 'tp'), may hold values from -0.125 to 0.125
- expert_down: bfloat16 [16, 1536, 2048], P('ep', 'tp'), may hold values from -0.15625 to 0.15625
- routing: int32 [1024, 2], P('ep'), may hold values from 0 to 15, all different within a row; in each aligned block of 64 rows (0 to 63, 64 to 127, ...) at most 16 rows name the same one
- route_scale: float32 [1024, 2], P('ep'), may hold values from 0.25 to 1
Outputs:
- layer_out: bfloat16 [1024, 2048], P('ep')
- new_state: float32 [1024, 16, 64, 64], P('ep', 'tp')
The draws below stay inside these ranges and needn't reach their ends.
Inputs may be any that keep to these rules, and one draw needn't show every extreme that they name: `routing`: among the 64 sequences of one index of ep, no expert is chosen more than 16 times, and some expert is chosen exactly 16 times; a sequence's 2 choices differ.
All inputs are finite; a program needn't handle non-finite values.
Results may differ from the reference program's by a relative error of at most 0.017.
Values may be sent and summed in bfloat16 or wider, within the bound.
A program may use at most 192 MiB of HBM per device.

```python
import math
import jax
import jax.numpy as jnp
import numpy as np
from jax import lax

D = 2048
HEADS = 16
HEAD = 64
LOW = 64
DFF = 5632
EFF = 1536
TOPK = 2
SEQS = 64
SEQUENCES = 1024
EXPERTS = 16
CAP = 16
N_EP = 16
N_TP = 2


def block_scale(stream_key, dims, pieces, least, largest):
    def one(position, blocks):
        steps = jax.random.uniform(jax.random.fold_in(jax.random.fold_in(stream_key, 6), position), (blocks,), jnp.float32, least / len(pieces), largest / len(pieces))
        return jnp.repeat(jnp.exp(steps), dims[position] // blocks).reshape((-1,) + (1,) * (len(dims) - position - 1))

    factor_of = one(*pieces[0])
    for cut in pieces[1:]:
        factor_of = factor_of * one(*cut)
    return factor_of


def assign_block(own_key, own, number, rows, number_of, top, most, lean):
    ranking = jax.random.permutation(own_key, number_of)
    packed, common = portions_of(number_of, rows * top, most, lean, True), portions_of(number_of, rows * top, most, lean, False)
    places = jnp.arange(number_of)

    def named(sizes, offset_by):
        used = int((sizes > 0).sum())
        fixed = max(1, used // 4)
        passed = fixed + (places - fixed + offset_by * (used - fixed)) % max(1, number_of - fixed)
        return jnp.zeros((number_of,), jnp.int32).at[ranking[jnp.where(places < fixed, places, passed)]].set(jnp.asarray(sizes, jnp.int32))

    sizes = jnp.where(number % 4 == 0, named(packed, number // 4), named(common, number - number // 4 - 1))
    mixed = jax.random.permutation(jax.random.fold_in(own, 3), number_of)
    donor, receiver = mixed[0:number_of // 2 * 2:2], mixed[1:number_of // 2 * 2:2]
    slack = jnp.minimum(sizes[donor] - 1, most - sizes[receiver]) // 2
    slack = jnp.where((donor == ranking[0]) | (receiver == ranking[0]) | (sizes[receiver] == 0), 0, jnp.maximum(slack, 0))
    passed = jax.random.randint(jax.random.fold_in(own, 4), (number_of // 2,), 0, 1 << 20) % (slack + 1)
    sizes = sizes.at[donor].add(-passed).at[receiver].add(passed)
    members = jnp.searchsorted(jnp.cumsum(sizes), jnp.arange(rows * top), side="right").astype(jnp.int32)
    listing = members.reshape(top, rows).T
    listing = listing[jax.random.permutation(jax.random.fold_in(own, 1), rows)]
    offset_by = jax.random.randint(jax.random.fold_in(own, 2), (rows, 1), 0, top)
    return jnp.take_along_axis(listing, (jnp.arange(top)[None, :] + offset_by) % top, axis=1)


def portions_of(count, total, most, lean, full):
    portions = [(1 << 20) // math.isqrt(grade ** lean) + 1 for grade in range(1, count + 1)]
    largest = most if full else min(most, max(-(-total // count), total * portions[0] // sum(portions)))
    least = 1 if total - largest >= count - 1 else 0
    counts, rest = [largest] + [least] * (count - 1), total - largest - least * (count - 1)
    while rest > 0:
        movable = [i for i in range(1, count) if counts[i] < largest] or [i for i in range(1, count) if counts[i] < most]
        pool, remaining = sum([portions[i] for i in movable]), rest
        for i in movable:
            extra = min(most - counts[i], max(1, remaining * portions[i] // pool), rest)
            counts[i] = counts[i] + extra
            rest = rest - extra
    return np.array(counts)


def scatter_about(key, shape, width, bound, pieces=(), held_as=jnp.bfloat16):
    values = jax.random.normal(key, shape, jnp.float32) * width
    if len(pieces) > 0:
        values = block_scale(key, shape, pieces, -0.22, 0.18) * values
    return jnp.clip(values, min=-bound, max=bound).astype(held_as)


def setup_inputs(seed: int = 0) -> dict:
    arg_keys = jax.random.split(jax.random.key(seed), 25)
    hidden = scatter_about(arg_keys[0], (SEQUENCES, D), 1.0, 6.0, ((0, 16),))
    mix_gain = jnp.clip(1.0 + 0.18 * jax.random.normal(arg_keys[1], (D,), jnp.float32), 0.1, 1.9)
    recept_weight = scatter_about(arg_keys[2], (D, HEADS * HEAD), D ** -0.5, 0.125, ((1, 2),))
    key_weight = scatter_about(arg_keys[3], (D, HEADS * HEAD), D ** -0.5, 0.125, ((1, 2),))
    value_weight = scatter_about(arg_keys[4], (D, HEADS * HEAD), D ** -0.5, 0.125, ((1, 2),))
    decay_down = scatter_about(arg_keys[5], (D, LOW), D ** -0.5, 0.125)
    decay_up = scatter_about(arg_keys[6], (LOW, HEADS * HEAD), LOW ** -0.5, 0.75)
    decay_bias = jnp.clip(jax.random.uniform(arg_keys[7], (HEADS * HEAD,), jnp.float32, -4.0, 1.0), -4.0, 1.0)
    rate_down = scatter_about(arg_keys[8], (D, LOW), D ** -0.5, 0.125)
    rate_up = scatter_about(arg_keys[9], (LOW, HEADS * HEAD), LOW ** -0.5, 0.75)
    rate_bias = scatter_about(arg_keys[10], (HEADS * HEAD,), 1.0, 4.0, (), jnp.float32)
    head_gain = jnp.clip(1.0 + 0.18 * jax.random.normal(arg_keys[11], (HEADS * HEAD,), jnp.float32), 0.1, 1.9)
    out_weight = scatter_about(arg_keys[12], (HEADS * HEAD, D), (HEADS * HEAD) ** -0.5, 0.1875, ((0, 2),))
    memory_state = scatter_about(arg_keys[13], (SEQUENCES, HEADS, HEAD, HEAD), 1.0, 6.0, ((0, 16), (1, 2)), jnp.float32)
    ffn_gain = jnp.clip(1.0 + 0.18 * jax.random.normal(arg_keys[14], (D,), jnp.float32), 0.1, 1.9)
    blend_vector = scatter_about(arg_keys[15], (D,), D ** -0.5, 0.125)
    dense_gate = scatter_about(arg_keys[16], (D, DFF), D ** -0.5, 0.125, ((1, 32),))
    dense_up = scatter_about(arg_keys[17], (D, DFF), D ** -0.5, 0.125, ((1, 32),))
    dense_down = scatter_about(arg_keys[18], (DFF, D), (DFF // 16) ** -0.5, 0.3125, ((0, 32),))
    expert_gate = scatter_about(arg_keys[19], (EXPERTS, D, EFF), D ** -0.5, 0.125, ((0, 16), (2, 2)))
    expert_up = scatter_about(arg_keys[20], (EXPERTS, D, EFF), D ** -0.5, 0.125, ((0, 16), (2, 2)))
    expert_down = scatter_about(arg_keys[21], (EXPERTS, EFF, D), EFF ** -0.5, 0.15625, ((0, 16), (1, 2)))
    routing_keys = jax.random.split(jax.random.fold_in(arg_keys[22], 1), SEQUENCES // SEQS)
    routing_turns = jax.random.permutation(jax.random.fold_in(arg_keys[22], 3), SEQUENCES // SEQS)
    routing = jax.vmap(lambda own, number: assign_block(jax.random.fold_in(arg_keys[22], 2), own, number, SEQS, EXPERTS, TOPK, CAP, 1))(routing_keys, routing_turns).reshape((SEQUENCES, TOPK))
    route_scale = jnp.clip(0.25 + 0.75 * jax.random.uniform(arg_keys[23], (SEQUENCES, TOPK), jnp.float32) ** block_scale(arg_keys[23], (SEQUENCES, TOPK), ((0, 16),), -0.2, 0.2), 0.25, 1.0)
    return {"hidden": hidden, "mix_gain": mix_gain, "recept_weight": recept_weight, "key_weight": key_weight, "value_weight": value_weight, "decay_down": decay_down, "decay_up": decay_up, "decay_bias": decay_bias, "rate_down": rate_down, "rate_up": rate_up, "rate_bias": rate_bias, "head_gain": head_gain, "out_weight": out_weight, "memory_state": memory_state, "ffn_gain": ffn_gain, "blend_vector": blend_vector, "dense_gate": dense_gate, "dense_up": dense_up, "dense_down": dense_down, "expert_gate": expert_gate, "expert_up": expert_up, "expert_down": expert_down, "routing": routing, "route_scale": route_scale}


def stored(tensor):
    return lax.optimization_barrier(tensor.astype(jnp.bfloat16)).astype(jnp.float32)

def rms_scaled(tensor, gain_vec):
    values = tensor.astype(jnp.float32)
    return values * lax.rsqrt(lax.optimization_barrier(jnp.mean(values * values, axis=-1, keepdims=True)) + 1e-06) * gain_vec

def silu_of(tensor):
    return tensor / (1.0 + jnp.exp(-tensor))

def matmul(left, right):
    return jnp.dot(left, right, preferred_element_type=jnp.float32)

def reference(hidden, mix_gain, recept_weight, key_weight, value_weight, decay_down, decay_up, decay_bias, rate_down, rate_up, rate_bias, head_gain, out_weight, memory_state, ffn_gain, blend_vector, dense_gate, dense_up, dense_down, expert_gate, expert_up, expert_down, routing, route_scale):
    seq_count = hidden.shape[0]
    full_width = HEADS * HEAD
    normed_in = rms_scaled(hidden, mix_gain).astype(jnp.bfloat16)
    recept_rows = stored(matmul(normed_in, recept_weight)).reshape(seq_count, HEADS, HEAD)
    key_rows = stored(matmul(normed_in, key_weight)).reshape(seq_count, HEADS, HEAD)
    value_rows = stored(matmul(normed_in, value_weight)).reshape(seq_count, HEADS, HEAD)
    decay_low = jnp.tanh(matmul(normed_in, decay_down)).astype(jnp.bfloat16)
    decay_pre = matmul(decay_low, decay_up) + decay_bias
    decay_rate = jnp.exp(-jnp.exp(-jax.nn.softplus(-decay_pre) - 0.5)).reshape(seq_count, HEADS, HEAD)
    rate_low = matmul(normed_in, rate_down).astype(jnp.bfloat16)
    learn_rate = jax.nn.sigmoid(matmul(rate_low, rate_up) + rate_bias).reshape(seq_count, HEADS, HEAD)
    unit_key = key_rows * lax.rsqrt(lax.optimization_barrier(jnp.sum(key_rows * key_rows, axis=-1, keepdims=True)) + 1e-06)
    removed = jnp.einsum('shij,shj->shi', memory_state, unit_key, precision=lax.Precision.HIGHEST)
    new_state = memory_state * decay_rate[:, :, None, :] - removed[..., None] * (unit_key * learn_rate)[:, :, None, :] + value_rows[..., None] * (key_rows * learn_rate)[:, :, None, :]
    readout = jnp.einsum('shij,shj->shi', new_state, recept_rows, precision=lax.Precision.HIGHEST)
    centre = lax.optimization_barrier(jnp.mean(readout, axis=-1, keepdims=True))
    variance = lax.optimization_barrier(jnp.mean(jnp.square(readout - centre), axis=-1, keepdims=True))
    head_normed = ((readout - centre) * lax.rsqrt(variance + 0.00064) * head_gain.reshape(HEADS, HEAD)).astype(jnp.bfloat16).reshape(seq_count, full_width)
    group_width = full_width // N_TP
    attn_sum = jnp.zeros((seq_count, D), jnp.float32)
    for group in range(N_TP):
        lower = group * group_width
        attn_sum = attn_sum + stored(matmul(head_normed[:, lower:lower + group_width], out_weight[lower:lower + group_width]))
    first_res = (hidden.astype(jnp.float32) + attn_sum).astype(jnp.bfloat16)
    ffn_in = rms_scaled(first_res, ffn_gain).astype(jnp.bfloat16)
    blend = jax.nn.sigmoid(jnp.dot(ffn_in, blend_vector, preferred_element_type=jnp.float32))
    dense_act = (silu_of(matmul(ffn_in, dense_gate)) * matmul(ffn_in, dense_up)).astype(jnp.bfloat16)
    dense_out = matmul(dense_act, dense_down)
    flat_route = routing.reshape(-1)
    flat_scale = route_scale.reshape(-1)
    slot_total = N_EP * CAP
    slot_index = jnp.arange(slot_total, dtype=jnp.int32)

    def one_expert(total, inputs):
        gate_mat, up_mat, down_mat, index = inputs
        chosen = flat_route == index
        live_count = jnp.sum(chosen.astype(jnp.int32))
        picks = jnp.nonzero(chosen, size=slot_total, fill_value=0)[0].astype(jnp.int32)
        owners = (picks // TOPK).astype(jnp.int32)
        rows = ffn_in[owners]
        live = slot_index < live_count
        scales = jnp.where(live, flat_scale[picks], jnp.zeros_like(flat_scale[picks]))
        expert_act = (silu_of(matmul(rows, gate_mat)) * matmul(rows, up_mat)).astype(jnp.bfloat16)
        expert_out = matmul(expert_act, down_mat)
        return (total.at[owners].add(expert_out * scales[:, None]), None)
    expert_sum, _ = lax.scan(one_expert, jnp.zeros((seq_count, D), jnp.float32), (expert_gate, expert_up, expert_down, jnp.arange(EXPERTS, dtype=jnp.int32)))
    layer_out = (first_res.astype(jnp.float32) + expert_sum + blend[:, None] * dense_out).astype(jnp.bfloat16)
    return (layer_out, new_state)
```

```python
import functools
import math

import jax
import jax.numpy as jnp
from jax import lax
from jax.experimental import pallas as pl
from jax.experimental.pallas import tpu as pltpu
from jax.sharding import PartitionSpec as P

MESH = pl.DeviceIdType.MESH
F32 = jnp.float32
BF16 = jnp.bfloat16
VMEM_LIMIT = 64 * 1024 * 1024 - 65536
VMEM_SPEC = pl.BlockSpec(memory_space=pltpu.VMEM)


def matmul(left, right):
    return jnp.dot(left, right, preferred_element_type=F32)


def matmul_nt(left, right):
    return lax.dot_general(left, right, (((1,), (1,)), ((), ())), preferred_element_type=F32)


def silu_of(tensor):
    return tensor / (1.0 + jnp.exp(-tensor))


def rms_scaled(values, gain):
    return values * lax.rsqrt(jnp.mean(values * values, axis=-1, keepdims=True) + 1e-06) * gain


def factors_of(count):
    slow = 4 if count % 4 == 0 else 1
    rest = count // slow
    mid = math.isqrt(rest)
    while rest % mid:
        mid -= 1
    return slow, mid, rest // mid


def attention_kernel(chunks, *refs):
    sources, (state_h, state_out_h, partial), rest = refs[:13], refs[13:16], refs[16:]
    local, rest = rest[:13], rest[13:]
    state_v, new_v, recept_s, pull_s, key_rate_s, value_s, decay_s, readout_s, normed_s = rest[:9]
    part_sem, in_sem, out_sem = rest[9:]
    (
        hidden,
        mix_gain,
        decay_down,
        rate_down,
        decay_up,
        rate_up,
        decay_bias,
        rate_bias,
        recept_weight,
        key_weight,
        value_weight,
        head_gain,
        out_weight,
    ) = local
    heads, seqs, size = pull_s.shape
    width = heads * size
    step_rows = seqs // chunks
    own = pl.ds(pl.multiple_of(lax.axis_index("tp") * width, 128), width)

    def part_copy(i):
        return pltpu.make_async_copy(sources[i], local[i], part_sem.at[i])

    def rows_of(c):
        return pl.ds(c * step_rows, step_rows)

    def in_copy(c):
        return pltpu.make_async_copy(state_h.at[rows_of(c)], state_v.at[rows_of(c)], in_sem.at[c])

    def out_copy(c):
        return pltpu.make_async_copy(new_v.at[rows_of(c)], state_out_h.at[rows_of(c)], out_sem.at[c])

    for i in range(11):
        part_copy(i).start()

    def start_in(c, carry):
        in_copy(c).start()
        return carry

    lax.fori_loop(0, chunks, start_in, 0)
    part_copy(11).start()
    part_copy(12).start()

    part_copy(0).wait()
    part_copy(1).wait()
    normed = rms_scaled(hidden[...].astype(F32), mix_gain[...]).astype(BF16)
    for i in range(2, 8):
        part_copy(i).wait()
    decay_low = jnp.tanh(matmul_nt(normed, decay_down[...])).astype(BF16)
    decay_pre = matmul(decay_low, decay_up[:, own]) + decay_bias[:, own]
    decay = jnp.exp(-math.exp(-0.5) / (1.0 + jnp.exp(-decay_pre)))
    rate_low = matmul_nt(normed, rate_down[...]).astype(BF16)
    rate = 1.0 / (1.0 + jnp.exp(-(matmul(rate_low, rate_up[:, own]) + rate_bias[:, own])))
    part_copy(8).wait()
    recept = matmul(normed, recept_weight[...]).astype(BF16).astype(F32)
    part_copy(9).wait()
    keys = matmul(normed, key_weight[...]).astype(BF16).astype(F32)
    part_copy(10).wait()
    vals = matmul(normed, value_weight[...]).astype(BF16).astype(F32)
    for h in range(heads):
        cols = slice(h * size, (h + 1) * size)
        key_h = keys[:, cols]
        inverse = 1.0 / (jnp.sum(key_h * key_h, axis=-1, keepdims=True) + 1e-06)
        recept_s[:, h, :] = recept[:, cols]
        pull_s[h] = key_h * inverse
        key_rate_s[h] = key_h * rate[:, cols]
        value_s[h] = vals[:, cols]
        decay_s[h] = decay[:, cols]

    shape, flat = (heads, size, size), (heads * size, size)
    eye = lax.broadcasted_iota(jnp.int32, shape, 1) == lax.broadcasted_iota(jnp.int32, shape, 2)
    spread = (heads, width)
    owner = lax.broadcasted_iota(jnp.int32, spread, 0)
    own_lanes = owner == lax.broadcasted_iota(jnp.int32, spread, 1) // size

    def one_sequence(row):
        here = pl.ds(row, 1)
        state = state_v[row]
        gain = jnp.sum(
            jnp.where(eye, value_s[:, here], 0.0) - state * pull_s[:, here], axis=-1, keepdims=True
        )
        new = state * decay_s[:, here] + gain * key_rate_s[:, here]
        new_v[row] = new
        out = matmul_nt(recept_s[row].astype(BF16), new.astype(BF16).reshape(flat))
        readout_s[here, :] = jnp.sum(jnp.where(own_lanes, out, 0.0), axis=0, keepdims=True)

    def one_chunk(c, carry):
        in_copy(c).wait()

        def some(k, inner):
            for j in range(4):
                one_sequence(c * step_rows + k * 4 + j)
            return inner

        lax.fori_loop(0, step_rows // 4, some, 0)
        out_copy(c).start()
        return carry

    lax.fori_loop(0, chunks, one_chunk, 0)

    part_copy(11).wait()
    gain = head_gain[:, own]
    for h in range(heads):
        cols = slice(h * size, (h + 1) * size)
        out = readout_s[:, cols]
        centred = out - jnp.mean(out, axis=-1, keepdims=True)
        variance = jnp.mean(centred * centred, axis=-1, keepdims=True)
        normed_s[:, cols] = (centred * lax.rsqrt(variance + 0.00064) * gain[:, cols]).astype(BF16)
    part_copy(12).wait()
    partial[...] = matmul(normed_s[...], out_weight[...]).astype(BF16)

    def wait_out(c, carry):
        out_copy(c).wait()
        return carry

    lax.fori_loop(0, chunks, wait_out, 0)


def attention(operands, state):
    seqs, heads, size, _ = state.shape
    hidden = operands[0]
    width = heads * size
    chunks = seqs // math.gcd(seqs, 8)
    per_head = pltpu.VMEM((heads, seqs, size), F32)
    dma = pltpu.SemaphoreType.DMA
    any_spec = pl.BlockSpec(memory_space=pl.ANY)
    return pl.pallas_call(
        functools.partial(attention_kernel, chunks),
        out_shape=(
            jax.ShapeDtypeStruct(state.shape, F32),
            jax.ShapeDtypeStruct(hidden.shape, BF16),
        ),
        in_specs=[any_spec] * 14,
        out_specs=(any_spec, VMEM_SPEC),
        scratch_shapes=[pltpu.VMEM(a.shape, a.dtype) for a in operands]
        + [
            pltpu.VMEM(state.shape, F32),
            pltpu.VMEM(state.shape, F32),
            pltpu.VMEM((seqs, heads, size), F32),
            per_head,
            per_head,
            per_head,
            per_head,
            pltpu.VMEM((seqs, width), F32),
            pltpu.VMEM((seqs, width), BF16),
            dma((13,)),
            dma((chunks,)),
            dma((chunks,)),
        ],
        compiler_params=pltpu.CompilerParams(vmem_limit_bytes=VMEM_LIMIT),
        name="attention",
    )(*operands, state)


def position(sizes):
    ep = lax.axis_index("ep")
    strides = (sizes[1] * sizes[2], sizes[2], 1)
    return ep, tuple(ep // s % n for s, n in zip(strides, sizes)), strides


def greet_all(count):
    ep, tp = lax.axis_index("ep"), lax.axis_index("tp")
    barrier = pltpu.get_barrier_semaphore()

    def greet(k, carry):
        pl.semaphore_signal(
            barrier, inc=1, device_id=((ep + k) % count, tp), device_id_type=MESH
        )
        return carry

    lax.fori_loop(1, count, greet, 0)
    pl.semaphore_signal(barrier, inc=1, device_id=(ep, 1 - tp), device_id_type=MESH)
    pl.semaphore_wait(barrier, count)


def remote(src, dst, send, recv, device):
    return pltpu.make_async_remote_copy(
        src_ref=src,
        dst_ref=dst,
        send_sem=send,
        recv_sem=recv,
        device_id=device,
        device_id_type=MESH,
    )


def gather_kernel(
    sizes,
    partial,
    hidden,
    gain,
    meta,
    first,
    tokens,
    metas,
    sibling_part,
    part_sem,
    meta_send,
    meta_recv,
    send_sem,
    recv_sem,
    pass_send,
    pass_recv,
):
    count = sizes[0] * sizes[1] * sizes[2]
    ep, at, strides = position(sizes)
    tp = lax.axis_index("tp")
    half = first.shape[0]
    mine = pl.ds(pl.multiple_of(tp * half, half), half)
    other = pl.ds(pl.multiple_of((1 - tp) * half, half), half)
    greet_all(count)
    swap = remote(partial.at[other], sibling_part, part_sem.at[0], part_sem.at[1], (ep, 1 - tp))
    swap.start()

    def meta_copy(k):
        return remote(
            meta, metas.at[ep], meta_send.at[k], meta_recv.at[k], ((ep + k) % count, tp)
        )

    def start_meta(k, carry):
        meta_copy(k).start()
        return carry

    lax.fori_loop(1, count, start_meta, 0)
    metas[ep] = meta[...]
    swap.wait()
    total = (
        hidden[mine, :].astype(F32)
        + partial[mine, :].astype(F32)
        + sibling_part[...].astype(F32)
    ).astype(BF16)
    first[...] = total
    ffn_in = rms_scaled(total.astype(F32), gain[...]).astype(BF16)
    tokens[at[0], at[1], at[2], mine, :] = ffn_in

    def views(order, r):
        _, d2, d3 = order

        def view(k, second, third):
            spot = [pl.ds((at[0] + sizes[0] - k) % sizes[0], 1), None, None]
            spot[d2], spot[d3] = second, third
            return tokens.at[tuple(spot) + (r,)]

        def one(d, j=0):
            return pl.ds((at[d] + sizes[d] - j) % sizes[d], 1)

        whole = pl.ds(0, sizes[d2])
        return (
            lambda k, j=0: view(k, one(d2), one(d3)),
            lambda k, j=0: view(k, one(d2, j), one(d3)),
            lambda k, j=0: view(k, whole, one(d3, j)),
        )

    def run(core, order, order_of_other):
        sibling = (ep, 1 - core)
        come = views(order, pl.ds(core * half, half))
        chunks = sizes[0]
        flights, passed = {}, []

        def send(stage, k, j):
            d = order[stage]
            source = come[stage](0 if stage == 0 else k)
            peer = ep + ((at[d] + j) % sizes[d] - at[d]) * strides[d]
            slot = (stage, k, j if stage else 0)
            copy = remote(source, source, send_sem.at[slot], recv_sem.at[slot], (peer, core))
            copy.start()
            flights[slot] = copy

        def onward(stage, k, j):
            view = come[stage](k, j)
            slot = (stage, k, j)
            copy = remote(view, view, pass_send.at[slot], pass_recv.at[slot], sibling)
            copy.start()
            passed.append(copy)

        def first_phase(k):
            if k:
                flights[0, k, 0].wait()
            for j in range(1, sizes[order[1]]):
                send(1, k, j)
            onward(0, k, 0)

        def later_phase(stage, k):
            for j in range(1, sizes[order[stage]]):
                flights[stage, k, j].wait()
            if stage == 1:
                for j in range(1, sizes[order[2]]):
                    send(2, k, j)
            for j in range(1, sizes[order[stage]]):
                onward(stage, k, j)

        first_phase(0)
        for k in range(1, chunks):
            send(0, k, k)
        for t in range(chunks + 2):
            if 0 <= t - 1 < chunks:
                later_phase(1, t - 1)
            if 0 < t < chunks:
                first_phase(t)
            if 0 <= t - 2 < chunks:
                later_phase(2, t - 2)
        for copy in passed:
            copy.wait_send()
        theirs = views(order_of_other, pl.ds((1 - core) * half, half))
        for stage in range(3):
            for k in range(chunks):
                for j in range(1, sizes[order_of_other[stage]]) if stage else (0,):
                    view, slot = theirs[stage](k, j), (stage, k, j)
                    remote(view, view, pass_send.at[slot], pass_recv.at[slot], sibling).wait_recv()

    @pl.when(tp == 0)
    def _():
        run(0, (0, 2, 1), (0, 1, 2))

    @pl.when(tp == 1)
    def _():
        run(1, (0, 1, 2), (0, 2, 1))

    def wait_meta(k, carry):
        meta_copy(k).wait()
        return carry

    lax.fori_loop(1, count, wait_meta, 0)


def gather_tokens(sizes, partial, hidden, gain, meta):
    seqs, width = hidden.shape
    count = sizes[0] * sizes[1] * sizes[2]
    half = seqs // 2
    most = max(sizes)
    dma = pltpu.SemaphoreType.DMA
    return pl.pallas_call(
        functools.partial(gather_kernel, sizes),
        out_shape=(
            jax.ShapeDtypeStruct((half, width), BF16),
            jax.ShapeDtypeStruct(sizes + (seqs, width), BF16),
            jax.ShapeDtypeStruct((count,) + meta.shape, F32),
        ),
        in_specs=[VMEM_SPEC] * 4,
        out_specs=(VMEM_SPEC,) * 3,
        scratch_shapes=[
            pltpu.VMEM((half, width), BF16),
            dma((2,)),
            dma((count,)),
            dma((count,)),
            dma((3, sizes[0], most)),
            dma((3, sizes[0], most)),
            dma((3, sizes[0], most)),
            dma((3, sizes[0], most)),
        ],
        compiler_params=pltpu.CompilerParams(
            collective_id=0, has_side_effects=True, vmem_limit_bytes=VMEM_LIMIT
        ),
        name="gather_tokens",
    )(partial, hidden, gain, meta)


def scatter_kernel(sizes, parts, first, out, total, from_sibling, land0, land1, sems):
    pair_send, pair_recv, send_sem, recv_sem, last_sem = sems
    ep, at, strides = position(sizes)
    tp = lax.axis_index("tp")
    half = first.shape[0]
    mine = pl.ds(pl.multiple_of(tp * half, half), half)
    other = pl.ds(pl.multiple_of((1 - tp) * half, half), half)
    chunks = sizes[0]
    goals = [(at[0] + 1 + k) % chunks for k in range(chunks)]
    greet_all(sizes[0] * sizes[1] * sizes[2])
    pairs = []
    for k in range(chunks):
        copy = remote(
            parts.at[goals[k], :, :, other],
            from_sibling.at[k],
            pair_send.at[k],
            pair_recv.at[k],
            (ep, 1 - tp),
        )
        copy.start()
        pairs.append(copy)

    def run(core, d1, d2, lands):
        rows = pl.ds(core * half, half)
        flights = {}

        def spot(k, c1, c2):
            place = [goals[k], None, None]
            place[d1], place[d2] = c1, c2
            return tuple(place)

        def send(stage, k, j, source, dst, d):
            peer = ep + ((at[d] + j) % sizes[d] - at[d]) * strides[d]
            slot = (stage, k, j if stage < 2 else 0)
            copy = remote(source, dst, send_sem.at[slot], recv_sem.at[slot], (peer, core))
            copy.start()
            flights[slot] = copy

        def pair_sum(k):
            pairs[k].wait()

            def add(b, carry):
                y, x = b // sizes[2], b % sizes[2]
                total[goals[k], y, x] = (
                    parts[goals[k], y, x, rows, :].astype(F32) + from_sibling[k, y, x].astype(F32)
                ).astype(BF16)
                return carry

            lax.fori_loop(0, sizes[1] * sizes[2], add, 0)
            for j in range(1, sizes[d1]):
                source = total.at[spot(k, (at[d1] + j) % sizes[d1], slice(None))]
                send(0, k, j, source, lands[0].at[k, j - 1], d1)

        def first_sum(k):
            for j in range(1, sizes[d1]):
                flights[0, k, j].wait()

            def add(b, carry):
                place = spot(k, at[d1], b)
                value = total[place].astype(F32)
                for j in range(1, sizes[d1]):
                    value = value + lands[0][k, j - 1, b].astype(F32)
                total[place] = value.astype(BF16)
                return carry

            lax.fori_loop(0, sizes[d2], add, 0)
            for j in range(1, sizes[d2]):
                source = total.at[spot(k, at[d1], (at[d2] + j) % sizes[d2])]
                send(1, k, j, source, lands[1].at[k, j - 1], d2)

        def second_sum(k):
            for j in range(1, sizes[d2]):
                flights[1, k, j].wait()
            place = spot(k, at[d1], at[d2])
            value = total[place].astype(F32)
            for j in range(1, sizes[d2]):
                value = value + lands[1][k, j - 1].astype(F32)
            if k < chunks - 1:
                total[place] = value.astype(BF16)
                send(2, k, k + 1, total.at[place], lands[2].at[k], 0)
                return
            value = value + first[...].astype(F32)
            for i in range(chunks - 1):
                flights[2, i, 0].wait()
                value = value + lands[2][i].astype(F32)
            out[rows, :] = value.astype(BF16)

        for t in range(chunks + 2):
            if t < chunks:
                pair_sum(t)
            if 0 <= t - 1 < chunks:
                first_sum(t - 1)
            if 0 <= t - 2 < chunks:
                second_sum(t - 2)

    @pl.when(tp == 0)
    def _():
        run(0, 1, 2, land0)

    @pl.when(tp == 1)
    def _():
        run(1, 2, 1, land1)

    swap = remote(out.at[mine], out.at[mine], last_sem.at[0], last_sem.at[1], (ep, 1 - tp))
    swap.start()
    swap.wait()


def landing(sizes, d1, d2, half, width):
    chunks, block = sizes[0], (half, width)
    return [
        pltpu.VMEM((chunks, max(1, sizes[d1] - 1), sizes[d2]) + block, BF16),
        pltpu.VMEM((chunks, max(1, sizes[d2] - 1)) + block, BF16),
        pltpu.VMEM((max(1, chunks - 1),) + block, BF16),
    ]


def scatter_sum(sizes, parts, first):
    half, width = first.shape
    most = max(sizes)
    dma = pltpu.SemaphoreType.DMA
    return pl.pallas_call(
        functools.partial(scatter_kernel, sizes),
        out_shape=jax.ShapeDtypeStruct((2 * half, width), BF16),
        in_specs=[VMEM_SPEC] * 2,
        out_specs=VMEM_SPEC,
        scratch_shapes=[
            pltpu.VMEM(sizes + (half, width), BF16),
            pltpu.VMEM(sizes + (half, width), BF16),
            landing(sizes, 1, 2, half, width),
            landing(sizes, 2, 1, half, width),
            [
                dma((sizes[0],)),
                dma((sizes[0],)),
                dma((3, sizes[0], most)),
                dma((3, sizes[0], most)),
                dma((2,)),
            ],
        ],
        compiler_params=pltpu.CompilerParams(
            collective_id=1, has_side_effects=True, vmem_limit_bytes=VMEM_LIMIT
        ),
        name="scatter_sum",
    )(parts, first)


def shards(
    hidden,
    mix_gain,
    recept_weight,
    key_weight,
    value_weight,
    decay_down,
    decay_up,
    decay_bias,
    rate_down,
    rate_up,
    rate_bias,
    head_gain,
    out_weight,
    memory_state,
    ffn_gain,
    blend_vector,
    dense_gate,
    dense_up,
    dense_down,
    expert_gate,
    expert_up,
    expert_down,
    routing,
    route_scale,
):
    seqs, width = hidden.shape
    count = lax.axis_size("ep")
    sizes = factors_of(count)
    top = routing.shape[1]
    cap = max(2, 2 * seqs * top // count)
    new_state, partial = attention(
        (
            hidden,
            mix_gain[None],
            decay_down.T,
            rate_down.T,
            decay_up,
            rate_up,
            decay_bias[None],
            rate_bias[None],
            recept_weight,
            key_weight,
            value_weight,
            head_gain[None],
            out_weight,
        ),
        memory_state,
    )
    meta = jnp.concatenate([routing.T.astype(F32), route_scale.T], axis=0)
    meta = jnp.pad(meta, ((0, -2 * top % 8), (0, -seqs % 128)))
    first, tokens, metas = gather_tokens(sizes, partial, hidden, ffn_gain[None], meta)
    tokens = tokens.reshape(count * seqs, width)

    hit = metas[:, :top, :seqs] == lax.axis_index("ep").astype(F32)
    chosen = jnp.any(hit, axis=1)
    scale_of = jnp.sum(jnp.where(hit, metas[:, top : 2 * top, :seqs], 0.0), axis=1)
    earlier = jnp.arange(seqs)[:, None] < jnp.arange(seqs)[None, :]
    rank = matmul(chosen.astype(BF16), earlier.astype(BF16)).astype(jnp.int32)
    place = jnp.where(chosen, rank + jnp.arange(count, dtype=jnp.int32)[:, None] * cap, -1)
    select = place.reshape(1, -1) == jnp.arange(count * cap, dtype=jnp.int32)[:, None]
    slot_scale = jnp.sum(jnp.where(select, scale_of.reshape(1, -1), 0.0), axis=1, keepdims=True)
    picked = matmul(select.astype(BF16), tokens).astype(BF16)
    expert_act = (silu_of(matmul(picked, expert_gate[0])) * matmul(picked, expert_up[0])).astype(BF16)
    expert_out = (matmul(expert_act, expert_down[0]) * slot_scale).astype(BF16)
    blend = jax.nn.sigmoid(matmul_nt(tokens, blend_vector[None]))
    dense_act = (
        silu_of(matmul(tokens, dense_gate)) * matmul(tokens, dense_up) * blend
    ).astype(BF16)
    spread = (place.reshape(-1, 1) == jnp.arange(count * cap, dtype=jnp.int32)[None, :]).astype(BF16)
    parts = matmul(
        jnp.concatenate([spread, dense_act], axis=1),
        jnp.concatenate([expert_out, dense_down], axis=0),
    ).astype(BF16)
    layer_out = scatter_sum(sizes, parts.reshape(sizes + (seqs, width)), first)
    return (layer_out, new_state)


def solution(mesh):
    in_specs = (
        P("ep", None),
        P(),
        P(None, "tp"),
        P(None, "tp"),
        P(None, "tp"),
        P(),
        P(),
        P(),
        P(),
        P(),
        P(),
        P(),
        P("tp", None),
        P("ep", "tp", None, None),
        P(),
        P(),
        P(None, ("ep", "tp")),
        P(None, ("ep", "tp")),
        P(("ep", "tp"), None),
        P("ep", None, "tp"),
        P("ep", None, "tp"),
        P("ep", "tp", None),
        P("ep", None),
        P("ep", None),
    )
    out_specs = (P("ep", None), P("ep", "tp", None, None))
    return jax.shard_map(shards, mesh=mesh, in_specs=in_specs, out_specs=out_specs, check_vma=False)
```

```python
import functools
import math

import jax
import jax.numpy as jnp
from jax import lax
from jax.experimental import pallas as pl
from jax.experimental.pallas import tpu as pltpu
from jax.sharding import PartitionSpec as P

MESH = pl.DeviceIdType.MESH
F32 = jnp.float32
BF16 = jnp.bfloat16
VMEM_LIMIT = 64 * 1024 * 1024 - 65536
VMEM_SPEC = pl.BlockSpec(memory_space=pltpu.VMEM)


def matmul(left, right):
    return jnp.dot(left, right, preferred_element_type=F32)


def matmul_nt(left, right):
    return lax.dot_general(left, right, (((1,), (1,)), ((), ())), preferred_element_type=F32)


def silu_of(tensor):
    return tensor / (1.0 + jnp.exp(-tensor))


def rms_scaled(values, gain):
    return values * lax.rsqrt(jnp.mean(values * values, axis=-1, keepdims=True) + 1e-06) * gain


def factors_of(count):
    slow = 4 if count % 4 == 0 else 1
    rest = count // slow
    mid = math.isqrt(rest)
    while rest % mid:
        mid -= 1
    return slow, mid, rest // mid


def attention_kernel(chunks, *refs):
    sources, (state_h, state_out_h, partial), rest = refs[:13], refs[13:16], refs[16:]
    local, rest = rest[:13], rest[13:]
    state_v, new_v, recept_s, pull_s, key_rate_s, value_s, decay_s, readout_s, normed_s = rest[:9]
    part_sem, in_sem, out_sem = rest[9:]
    (
        hidden,
        mix_gain,
        decay_down,
        rate_down,
        decay_up,
        rate_up,
        decay_bias,
        rate_bias,
        recept_weight,
        key_weight,
        value_weight,
        head_gain,
        out_weight,
    ) = local
    heads, seqs, size = pull_s.shape
    width = heads * size
    step_rows = seqs // chunks
    own = pl.ds(pl.multiple_of(lax.axis_index("tp") * width, 128), width)

    def part_copy(i):
        return pltpu.make_async_copy(sources[i], local[i], part_sem.at[i])

    def rows_of(c):
        return pl.ds(c * step_rows, step_rows)

    def in_copy(c):
        return pltpu.make_async_copy(state_h.at[rows_of(c)], state_v.at[rows_of(c)], in_sem.at[c])

    def out_copy(c):
        return pltpu.make_async_copy(new_v.at[rows_of(c)], state_out_h.at[rows_of(c)], out_sem.at[c])

    for i in range(11):
        part_copy(i).start()

    def start_in(c, carry):
        in_copy(c).start()
        return carry

    lax.fori_loop(0, chunks, start_in, 0)
    part_copy(11).start()
    part_copy(12).start()

    part_copy(0).wait()
    part_copy(1).wait()
    normed = rms_scaled(hidden[...].astype(F32), mix_gain[...]).astype(BF16)
    for i in range(2, 8):
        part_copy(i).wait()
    decay_low = jnp.tanh(matmul_nt(normed, decay_down[...])).astype(BF16)
    decay_pre = matmul(decay_low, decay_up[:, own]) + decay_bias[:, own]
    decay = jnp.exp(-math.exp(-0.5) / (1.0 + jnp.exp(-decay_pre)))
    rate_low = matmul_nt(normed, rate_down[...]).astype(BF16)
    rate = 1.0 / (1.0 + jnp.exp(-(matmul(rate_low, rate_up[:, own]) + rate_bias[:, own])))
    part_copy(8).wait()
    recept = matmul(normed, recept_weight[...]).astype(BF16).astype(F32)
    part_copy(9).wait()
    keys = matmul(normed, key_weight[...]).astype(BF16).astype(F32)
    part_copy(10).wait()
    vals = matmul(normed, value_weight[...]).astype(BF16).astype(F32)
    for h in range(heads):
        cols = slice(h * size, (h + 1) * size)
        key_h = keys[:, cols]
        inverse = 1.0 / (jnp.sum(key_h * key_h, axis=-1, keepdims=True) + 1e-06)
        recept_s[:, h, :] = recept[:, cols]
        pull_s[h] = key_h * inverse
        key_rate_s[h] = key_h * rate[:, cols]
        value_s[h] = vals[:, cols]
        decay_s[h] = decay[:, cols]

    shape, flat = (heads, size, size), (heads * size, size)
    eye = lax.broadcasted_iota(jnp.int32, shape, 1) == lax.broadcasted_iota(jnp.int32, shape, 2)
    spread = (heads, width)
    owner = lax.broadcasted_iota(jnp.int32, spread, 0)
    own_lanes = owner == lax.broadcasted_iota(jnp.int32, spread, 1) // size

    def one_sequence(row):
        here = pl.ds(row, 1)
        state = state_v[row]
        gain = jnp.sum(
            jnp.where(eye, value_s[:, here], 0.0) - state * pull_s[:, here], axis=-1, keepdims=True
        )
        new = state * decay_s[:, here] + gain * key_rate_s[:, here]
        new_v[row] = new
        out = matmul_nt(recept_s[row].astype(BF16), new.astype(BF16).reshape(flat))
        readout_s[here, :] = jnp.sum(jnp.where(own_lanes, out, 0.0), axis=0, keepdims=True)

    def one_chunk(c, carry):
        in_copy(c).wait()

        def some(k, inner):
            for j in range(4):
                one_sequence(c * step_rows + k * 4 + j)
            return inner

        lax.fori_loop(0, step_rows // 4, some, 0)
        out_copy(c).start()
        return carry

    lax.fori_loop(0, chunks, one_chunk, 0)

    part_copy(11).wait()
    gain = head_gain[:, own]
    for h in range(heads):
        cols = slice(h * size, (h + 1) * size)
        out = readout_s[:, cols]
        centred = out - jnp.mean(out, axis=-1, keepdims=True)
        variance = jnp.mean(centred * centred, axis=-1, keepdims=True)
        normed_s[:, cols] = (centred * lax.rsqrt(variance + 0.00064) * gain[:, cols]).astype(BF16)
    part_copy(12).wait()
    partial[...] = matmul(normed_s[...], out_weight[...]).astype(BF16)

    def wait_out(c, carry):
        out_copy(c).wait()
        return carry

    lax.fori_loop(0, chunks, wait_out, 0)


def attention(operands, state):
    seqs, heads, size, _ = state.shape
    hidden = operands[0]
    width = heads * size
    chunks = seqs // math.gcd(seqs, 8)
    per_head = pltpu.VMEM((heads, seqs, size), F32)
    dma = pltpu.SemaphoreType.DMA
    any_spec = pl.BlockSpec(memory_space=pl.ANY)
    return pl.pallas_call(
        functools.partial(attention_kernel, chunks),
        out_shape=(
            jax.ShapeDtypeStruct(state.shape, F32),
            jax.ShapeDtypeStruct(hidden.shape, BF16),
        ),
        in_specs=[any_spec] * 14,
        out_specs=(any_spec, VMEM_SPEC),
        scratch_shapes=[pltpu.VMEM(a.shape, a.dtype) for a in operands]
        + [
            pltpu.VMEM(state.shape, F32),
            pltpu.VMEM(state.shape, F32),
            pltpu.VMEM((seqs, heads, size), F32),
            per_head,
            per_head,
            per_head,
            per_head,
            pltpu.VMEM((seqs, width), F32),
            pltpu.VMEM((seqs, width), BF16),
            dma((13,)),
            dma((chunks,)),
            dma((chunks,)),
        ],
        compiler_params=pltpu.CompilerParams(vmem_limit_bytes=VMEM_LIMIT),
        name="attention",
    )(*operands, state)


def position(sizes):
    ep = lax.axis_index("ep")
    strides = (sizes[1] * sizes[2], sizes[2], 1)
    return ep, tuple(ep // s % n for s, n in zip(strides, sizes)), strides


def greet_all(count):
    ep, tp = lax.axis_index("ep"), lax.axis_index("tp")
    barrier = pltpu.get_barrier_semaphore()

    def greet(k, carry):
        pl.semaphore_signal(
            barrier, inc=1, device_id=((ep + k) % count, tp), device_id_type=MESH
        )
        return carry

    lax.fori_loop(1, count, greet, 0)
    pl.semaphore_signal(barrier, inc=1, device_id=(ep, 1 - tp), device_id_type=MESH)
    pl.semaphore_wait(barrier, count)


def remote(src, dst, send, recv, device):
    return pltpu.make_async_remote_copy(
        src_ref=src,
        dst_ref=dst,
        send_sem=send,
        recv_sem=recv,
        device_id=device,
        device_id_type=MESH,
    )


def layer_kernel(
    sizes,
    top,
    cap,
    partial,
    hidden,
    gain,
    blend_vector,
    routing,
    route_scale,
    gate_h,
    up_h,
    down_h,
    expert_gate_h,
    expert_up_h,
    expert_down_h,
    out,
    tokens,
    metas,
    meta,
    first,
    sibling_part,
    gate_v,
    up_v,
    down_v,
    expert_gate,
    expert_up,
    expert_down,
    gate_w,
    up_w,
    mix_w,
    mix_rows,
    picked,
    expert_act,
    slot_scale,
    from_sibling,
    lands,
    sems,
):
    (
        weight_sem,
        part_sem,
        meta_send,
        meta_recv,
        ag_send,
        ag_recv,
        pass_send,
        pass_recv,
        pair_send,
        pair_recv,
        rs_send,
        rs_recv,
        last_sem,
    ) = sems
    chunks, across, along = sizes
    count = chunks * across * along
    plane = across * along
    ep, at, strides = position(sizes)
    tp = lax.axis_index("tp")
    half, width = first.shape
    seqs = 2 * half
    sibling = (ep, 1 - tp)
    mine = pl.ds(pl.multiple_of(tp * half, half), half)
    other = pl.ds(pl.multiple_of((1 - tp) * half, half), half)
    slots = plane * cap
    depth = gate_w.shape[0]
    units = gate_v.shape[0]
    rows_at_once = max(1, 256 // (along * seqs))
    blocks = across // rows_at_once
    block_chips = rows_at_once * along
    block_rows = block_chips * seqs
    tile = 256

    weights = (
        (gate_h, gate_v),
        (up_h, up_v),
        (down_h, down_v),
        (expert_gate_h, expert_gate),
        (expert_up_h, expert_up),
        (expert_down_h, expert_down),
    )

    def weight_copy(i):
        return pltpu.make_async_copy(weights[i][0], weights[i][1], weight_sem.at[i])

    def per_core(run):
        @pl.when(tp == 0)
        def _():
            run(0)

        @pl.when(tp == 1)
        def _():
            run(1)

    def meta_copy(k):
        peer = (ep + k) % count
        place = metas.at[at[0], at[1] * along + at[2]]
        return remote(meta, place, meta_send.at[k], meta_recv.at[k], (peer, tp))

    for i in range(6):
        weight_copy(i).start()
    greet_all(count)
    swap = remote(partial.at[other], sibling_part, part_sem.at[0], part_sem.at[1], sibling)
    swap.start()
    meta[...] = jnp.zeros(meta.shape, F32)
    meta[0:top, 0:seqs] = routing[...].astype(F32)
    meta[top : 2 * top, 0:seqs] = route_scale[...]
    base = hidden[mine, :].astype(F32) + partial[mine, :].astype(F32)
    swap.wait()
    total = (base + sibling_part[...].astype(F32)).astype(BF16)
    first[...] = total
    tokens[at[0], at[1], at[2], mine, :] = rms_scaled(total.astype(F32), gain[...]).astype(BF16)

    gather_orders = ((0, 2, 1), (0, 1, 2))

    def gather_view(core, stage, k, j):
        _, d2, d3 = gather_orders[core]
        spot = [pl.ds((at[0] + chunks - k) % chunks, 1), None, None]

        def one(d, back=0):
            return pl.ds((at[d] + sizes[d] - back) % sizes[d], 1)

        spot[d2] = pl.ds(0, sizes[d2]) if stage == 2 else one(d2, j if stage == 1 else 0)
        spot[d3] = one(d3, j if stage == 2 else 0)
        return tokens.at[tuple(spot) + (pl.ds(core * half, half),)]

    def gather_copy(core, stage, k, j):
        d = gather_orders[core][stage]
        source = gather_view(core, stage, 0 if stage == 0 else k, 0)
        peer = ep + ((at[d] + j) % sizes[d] - at[d]) * strides[d]
        slot = (stage, k, j if stage else 0)
        return remote(source, source, ag_send.at[slot], ag_recv.at[slot], (peer, core))

    def pass_copy(core, stage, k, j):
        view, slot = gather_view(core, stage, k, j), (stage, k, j)
        return remote(view, view, pass_send.at[slot], pass_recv.at[slot], sibling)

    def pass_slots(core, k):
        yield 0, k, 0
        for stage in (1, 2):
            for j in range(1, sizes[gather_orders[core][stage]]):
                yield stage, k, j

    def gather_begin(core):
        for j in range(1, sizes[gather_orders[core][1]]):
            gather_copy(core, 1, 0, j).start()
        for k in range(1, chunks):
            gather_copy(core, 0, k, k).start()
        pass_copy(core, 0, 0, 0).start()

    def gather_step(core, t):
        order = gather_orders[core]

        def later_phase(stage, k):
            for j in range(1, sizes[order[stage]]):
                gather_copy(core, stage, k, j).wait()
            if stage == 1:
                for j in range(1, sizes[order[2]]):
                    gather_copy(core, 2, k, j).start()
            for j in range(1, sizes[order[stage]]):
                pass_copy(core, stage, k, j).start()

        if 0 <= t - 1 < chunks:
            later_phase(1, t - 1)
        if 0 < t < chunks:
            gather_copy(core, 0, t, t).wait()
            for j in range(1, sizes[order[1]]):
                gather_copy(core, 1, t, j).start()
            pass_copy(core, 0, t, 0).start()
        if 0 <= t - 2 < chunks:
            later_phase(2, t - 2)

    per_core(gather_begin)

    def start_meta(k, carry):
        meta_copy(k).start()
        return carry

    def wait_meta(k, carry):
        meta_copy(k).wait()
        return carry

    lax.fori_loop(1, count, start_meta, 0)
    metas[at[0], at[1] * along + at[2]] = meta[...]

    for i in range(3):
        weight_copy(i).wait()
    top_row = lax.broadcasted_iota(jnp.int32, (slots, width), 0) == 0
    gate_w[0:slots, :] = jnp.where(top_row, blend_vector[...].astype(F32), 0.0).astype(BF16)
    up_w[0:slots, :] = jnp.zeros((slots, width), BF16)
    if slots + units < depth:
        rest = (depth - slots - units, width)
        gate_w[slots + units : depth, :] = jnp.zeros(rest, BF16)
        up_w[slots + units : depth, :] = jnp.zeros(rest, BF16)
    gate_w[slots : slots + units, :] = gate_v[...]
    up_w[slots : slots + units, :] = up_v[...]

    def fill(z, carry):
        if slots + units < depth:
            mix_w[z, slots + units : depth, :] = jnp.zeros((depth - slots - units, width), BF16)
        mix_w[z, slots : slots + units, :] = down_v[...]
        return carry

    lax.fori_loop(0, chunks, fill, 0)

    def plane_of(k):
        return (at[0] + chunks - k) % chunks

    def use_tokens(k):
        z = plane_of(k)

        def arrive(core):
            for slot in pass_slots(1 - core, k):
                pass_copy(1 - core, *slot).wait_recv()

        per_core(arrive)
        here = metas[z]
        lanes = lax.broadcasted_iota(jnp.int32, (plane, 128), 1)
        expert = ep.astype(F32)
        chosen = jnp.zeros((plane, 128), F32)
        scale_of = jnp.zeros((plane, 128), F32)
        for c in range(top):
            hit = jnp.where((here[:, c, :] == expert) & (lanes < seqs), 1.0, 0.0)
            chosen = chosen + hit
            scale_of = scale_of + hit * here[:, top + c, :]
        earlier = lax.broadcasted_iota(jnp.int32, (128, 128), 0) < lax.broadcasted_iota(
            jnp.int32, (128, 128), 1
        )
        rank = matmul(chosen.astype(BF16), jnp.where(earlier, 1.0, 0.0).astype(BF16))
        chip = lax.broadcasted_iota(jnp.int32, (plane, 128), 0).astype(F32)
        place = jnp.where(chosen > 0.5, rank + chip * cap, -1.0)
        scales = jnp.zeros((slots, 1), F32)
        for i in range(blocks):
            chips = range(i * block_chips, (i + 1) * block_chips)
            place_row = jnp.concatenate([place[p : p + 1, :seqs] for p in chips], axis=1)
            scale_row = jnp.concatenate([scale_of[p : p + 1, :seqs] for p in chips], axis=1)
            slot_of = lax.broadcasted_iota(jnp.int32, (depth, block_rows), 0).astype(F32)
            select = jnp.where(slot_of == place_row, 1.0, 0.0)
            scales = scales + jnp.sum(select[:slots] * scale_row, axis=1, keepdims=True)
            ys = pl.ds(i * rows_at_once, rows_at_once)
            own_slots = slice(i * block_chips * cap, (i + 1) * block_chips * cap)
            part = select[own_slots].astype(BF16)

            def pick(n, carry):
                cols = pl.ds(pl.multiple_of(n * tile, tile), tile)
                found = matmul(part, tokens[z, ys, :, :, cols].reshape(block_rows, tile))
                picked[z, own_slots, cols] = found.astype(BF16)
                return carry

            lax.fori_loop(0, width // tile, pick, 0)
            own_rows = slice(i * block_rows, (i + 1) * block_rows)
            mix_rows[z, own_rows, :] = jnp.transpose(select).astype(BF16)
        slot_scale[z] = jnp.broadcast_to(scales, (slots, 128))

        def dense(i, carry):
            rows = tokens[z, pl.ds(i * rows_at_once, rows_at_once)].reshape(block_rows, width)
            gate = matmul_nt(rows, gate_w[...])
            blend = 1.0 / (1.0 + jnp.exp(-gate[:, 0:1]))
            act = silu_of(gate) * matmul_nt(rows, up_w[...]) * blend
            own_rows = pl.ds(pl.multiple_of(i * block_rows, block_rows), block_rows)
            mix_rows[z, own_rows, :] = (mix_rows[z, own_rows, :].astype(F32) + act).astype(BF16)
            return carry

        lax.fori_loop(0, blocks, dense, 0)

    for t in range(chunks + 2):
        per_core(functools.partial(gather_step, t=t))
        if t == 2:
            lax.fori_loop(1, count, wait_meta, 0)
        if t >= 3:
            use_tokens(t - 3)
    use_tokens(chunks - 1)

    def passes_done(core):
        for k in range(chunks):
            for slot in pass_slots(core, k):
                pass_copy(core, *slot).wait_send()

    per_core(passes_done)

    for i in range(3, 6):
        weight_copy(i).wait()
    slots_all = chunks * slots

    def expert_hidden(n, carry):
        cols = pl.ds(pl.multiple_of(n * tile, tile), tile)
        rows = picked[...].reshape(slots_all, width)
        gate = matmul(rows, expert_gate[0, :, cols])
        expert_act[:, cols] = (silu_of(gate) * matmul(rows, expert_up[0, :, cols])).astype(BF16)
        return carry

    lax.fori_loop(0, expert_gate.shape[2] // tile, expert_hidden, 0)
    scale_all = slot_scale[...].reshape(slots_all, 128)[:, 0:1]

    def expert_result(n, carry):
        cols = pl.ds(pl.multiple_of(n * tile, tile), tile)
        result = (matmul(expert_act[...], expert_down[0, :, cols]) * scale_all).astype(BF16)
        for z in range(chunks):
            mix_w[z, 0:slots, cols] = result[z * slots : (z + 1) * slots]
        return carry

    lax.fori_loop(0, width // tile, expert_result, 0)

    goals = [(at[0] + 1 + k) % chunks for k in range(chunks)]
    scatter_orders = ((1, 2), (2, 1))

    def pair_copy(k):
        return remote(
            tokens.at[goals[k], :, :, other],
            from_sibling.at[k],
            pair_send.at[k],
            pair_recv.at[k],
            sibling,
        )

    def make_part(k):
        z = goals[k]

        def some(n, carry):
            cols = pl.ds(pl.multiple_of(n * tile, tile), tile)
            for i in range(blocks):
                own_rows = slice(i * block_rows, (i + 1) * block_rows)
                part = matmul(mix_rows[z, own_rows, :], mix_w[z, :, cols]).astype(BF16)
                ys = pl.ds(i * rows_at_once, rows_at_once)
                tokens[z, ys, :, :, cols] = part.reshape(rows_at_once, along, seqs, tile)
            return carry

        lax.fori_loop(0, width // tile, some, 0)
        pair_copy(k).start()

    def spot(core, k, c1, c2):
        d1, d2 = scatter_orders[core]
        place = [goals[k], None, None]
        place[d1], place[d2] = c1, c2
        return tuple(place) + (pl.ds(core * half, half),)

    def scatter_copy(core, stage, k, j):
        d1, d2 = scatter_orders[core]
        if stage == 0:
            d = d1
            source = tokens.at[spot(core, k, (at[d1] + j) % sizes[d1], slice(None))]
            target = lands[0].at[k, j - 1]
        elif stage == 1:
            d = d2
            source = tokens.at[spot(core, k, at[d1], (at[d2] + j) % sizes[d2])]
            target = lands[1].at[k, j - 1]
        else:
            d = 0
            source = tokens.at[spot(core, k, at[d1], at[d2])]
            target = lands[2].at[k]
        peer = ep + ((at[d] + j) % sizes[d] - at[d]) * strides[d]
        slot = (stage, k, j if stage < 2 else 0)
        return remote(source, target, rs_send.at[slot], rs_recv.at[slot], (peer, core))

    def pair_sum(k):
        pair_copy(k).wait()

        def add(b, carry):
            y, x = b // along, b % along
            tokens[goals[k], y, x, mine, :] = (
                tokens[goals[k], y, x, mine, :].astype(F32) + from_sibling[k, y, x].astype(F32)
            ).astype(BF16)
            return carry

        lax.fori_loop(0, plane, add, 0)

        def send(core):
            for j in range(1, sizes[scatter_orders[core][0]]):
                scatter_copy(core, 0, k, j).start()

        per_core(send)

    def first_sum(core, k):
        d1, d2 = scatter_orders[core]
        for j in range(1, sizes[d1]):
            scatter_copy(core, 0, k, j).wait()

        def add(b, carry):
            place = spot(core, k, at[d1], b)
            value = tokens[place].astype(F32)
            for j in range(1, sizes[d1]):
                value = value + lands[0][k, j - 1, b].astype(F32)
            tokens[place] = value.astype(BF16)
            return carry

        lax.fori_loop(0, sizes[d2], add, 0)
        for j in range(1, sizes[d2]):
            scatter_copy(core, 1, k, j).start()

    def second_sum(core, k):
        d1, d2 = scatter_orders[core]
        for j in range(1, sizes[d2]):
            scatter_copy(core, 1, k, j).wait()
        place = spot(core, k, at[d1], at[d2])
        value = tokens[place].astype(F32)
        for j in range(1, sizes[d2]):
            value = value + lands[1][k, j - 1].astype(F32)
        if k < chunks - 1:
            tokens[place] = value.astype(BF16)
            scatter_copy(core, 2, k, k + 1).start()
            return
        value = value + first[...].astype(F32)
        for i in range(chunks - 1):
            scatter_copy(core, 2, i, i + 1).wait()
            value = value + lands[2][i].astype(F32)
        out[pl.ds(core * half, half), :] = value.astype(BF16)

    for t in range(chunks + 3):
        if t < chunks:
            make_part(t)
        if 0 <= t - 1 < chunks:
            pair_sum(t - 1)
        if 0 <= t - 2 < chunks:
            per_core(functools.partial(first_sum, k=t - 2))
        if 0 <= t - 3 < chunks:
            per_core(functools.partial(second_sum, k=t - 3))

    last = remote(out.at[mine], out.at[mine], last_sem.at[0], last_sem.at[1], sibling)
    last.start()
    last.wait()


def layer_after(sizes, partial, hidden, gain, blend_vector, routing, route_scale, weights):
    seqs, width = hidden.shape
    count = sizes[0] * sizes[1] * sizes[2]
    half, top, most = seqs // 2, routing.shape[0], max(sizes)
    cap = max(2, 2 * seqs * top // count)
    plane = sizes[1] * sizes[2]
    slots = plane * cap
    depth = -(-(slots + weights[0].shape[0]) // 128) * 128
    chunks, side, block = sizes[0], max(sizes[1:]), (half, width)
    dma = pltpu.SemaphoreType.DMA
    any_spec = pl.BlockSpec(memory_space=pl.ANY)
    hop = dma((3, chunks, most))
    return pl.pallas_call(
        functools.partial(layer_kernel, sizes, top, cap),
        out_shape=jax.ShapeDtypeStruct((seqs, width), BF16),
        in_specs=[VMEM_SPEC] * 6 + [any_spec] * 6,
        out_specs=VMEM_SPEC,
        scratch_shapes=[
            pltpu.VMEM(sizes + (seqs, width), BF16),
            pltpu.VMEM((chunks, plane, 8, 128), F32),
            pltpu.VMEM((8, 128), F32),
            pltpu.VMEM(block, BF16),
            pltpu.VMEM(block, BF16),
        ]
        + [pltpu.VMEM(w.shape, BF16) for w in weights]
        + [
            pltpu.VMEM((depth, width), BF16),
            pltpu.VMEM((depth, width), BF16),
            pltpu.VMEM((chunks, depth, width), BF16),
            pltpu.VMEM((chunks, plane * seqs, depth), BF16),
            pltpu.VMEM((chunks, slots, width), BF16),
            pltpu.VMEM((chunks * slots, weights[3].shape[2]), BF16),
            pltpu.VMEM((chunks, slots, 128), F32),
            pltpu.VMEM(sizes + block, BF16),
            [
                pltpu.VMEM((chunks, max(1, side - 1), side) + block, BF16),
                pltpu.VMEM((chunks, max(1, side - 1)) + block, BF16),
                pltpu.VMEM((max(1, chunks - 1),) + block, BF16),
            ],
            [
                dma((6,)),
                dma((2,)),
                dma((count,)),
                dma((count,)),
                hop,
                hop,
                hop,
                hop,
                dma((chunks,)),
                dma((chunks,)),
                hop,
                hop,
                dma((2,)),
            ],
        ],
        compiler_params=pltpu.CompilerParams(
            collective_id=0, has_side_effects=True, vmem_limit_bytes=VMEM_LIMIT
        ),
        name="layer_after",
    )(partial, hidden, gain, blend_vector, routing, route_scale, *weights)


def shards(
    hidden,
    mix_gain,
    recept_weight,
    key_weight,
    value_weight,
    decay_down,
    decay_up,
    decay_bias,
    rate_down,
    rate_up,
    rate_bias,
    head_gain,
    out_weight,
    memory_state,
    ffn_gain,
    blend_vector,
    dense_gate,
    dense_up,
    dense_down,
    expert_gate,
    expert_up,
    expert_down,
    routing,
    route_scale,
):
    sizes = factors_of(lax.axis_size("ep"))
    new_state, partial = attention(
        (
            hidden,
            mix_gain[None],
            decay_down.T,
            rate_down.T,
            decay_up,
            rate_up,
            decay_bias[None],
            rate_bias[None],
            recept_weight,
            key_weight,
            value_weight,
            head_gain[None],
            out_weight,
        ),
        memory_state,
    )
    layer_out = layer_after(
        sizes,
        partial,
        hidden,
        ffn_gain[None],
        blend_vector[None],
        routing.T,
        route_scale.T,
        (dense_gate.T, dense_up.T, dense_down, expert_gate, expert_up, expert_down),
    )
    return (layer_out, new_state)


def solution(mesh):
    in_specs = (
        P("ep", None),
        P(),
        P(None, "tp"),
        P(None, "tp"),
        P(None, "tp"),
        P(),
        P(),
        P(),
        P(),
        P(),
        P(),
        P(),
        P("tp", None),
        P("ep", "tp", None, None),
        P(),
        P(),
        P(None, ("ep", "tp")),
        P(None, ("ep", "tp")),
        P(("ep", "tp"), None),
        P("ep", None, "tp"),
        P("ep", None, "tp"),
        P("ep", "tp", None),
        P("ep", None),
        P("ep", None),
    )
    out_specs = (P("ep", None), P("ep", "tp", None, None))
    return jax.shard_map(shards, mesh=mesh, in_specs=in_specs, out_specs=out_specs, check_vma=False)
```

```python
import functools
import math

import jax
import jax.numpy as jnp
from jax import lax
from jax.experimental import pallas as pl
from jax.experimental.pallas import tpu as pltpu
from jax.sharding import PartitionSpec as P

MESH = pl.DeviceIdType.MESH
F32 = jnp.float32
BF16 = jnp.bfloat16
VMEM_LIMIT = 64 * 1024 * 1024 - 65536
VMEM_SPEC = pl.BlockSpec(memory_space=pltpu.VMEM)


def matmul(left, right):
    return jnp.dot(left, right, preferred_element_type=F32)


def matmul_nt(left, right):
    return lax.dot_general(left, right, (((1,), (1,)), ((), ())), preferred_element_type=F32)


def silu_of(tensor):
    return tensor / (1.0 + jnp.exp(-tensor))


def rms_scaled(values, gain):
    return values * lax.rsqrt(jnp.mean(values * values, axis=-1, keepdims=True) + 1e-06) * gain


def factors_of(count):
    slow = 4 if count % 4 == 0 else 1
    rest = count // slow
    mid = math.isqrt(rest)
    while rest % mid:
        mid -= 1
    return slow, mid, rest // mid


def attention_kernel(chunks, *refs):
    sources, (state_h, state_out_h, partial), rest = refs[:13], refs[13:16], refs[16:]
    local, rest = rest[:13], rest[13:]
    state_v, new_v, recept_s, pull_s, key_rate_s, value_s, decay_s, readout_s, normed_s = rest[:9]
    part_sem, in_sem, out_sem = rest[9:]
    (
        hidden,
        mix_gain,
        decay_down,
        rate_down,
        decay_up,
        rate_up,
        decay_bias,
        rate_bias,
        recept_weight,
        key_weight,
        value_weight,
        head_gain,
        out_weight,
    ) = local
    heads, seqs, size = pull_s.shape
    width = heads * size
    step_rows = seqs // chunks
    own = pl.ds(pl.multiple_of(lax.axis_index("tp") * width, 128), width)

    def part_copy(i):
        return pltpu.make_async_copy(sources[i], local[i], part_sem.at[i])

    def rows_of(c):
        return pl.ds(c * step_rows, step_rows)

    def in_copy(c):
        return pltpu.make_async_copy(state_h.at[rows_of(c)], state_v.at[rows_of(c)], in_sem.at[c])

    def out_copy(c):
        return pltpu.make_async_copy(new_v.at[rows_of(c)], state_out_h.at[rows_of(c)], out_sem.at[c])

    for i in range(11):
        part_copy(i).start()

    def start_in(c, carry):
        in_copy(c).start()
        return carry

    lax.fori_loop(0, chunks, start_in, 0)
    part_copy(11).start()
    part_copy(12).start()

    part_copy(0).wait()
    part_copy(1).wait()
    normed = rms_scaled(hidden[...].astype(F32), mix_gain[...]).astype(BF16)
    for i in range(2, 8):
        part_copy(i).wait()
    decay_low = jnp.tanh(matmul_nt(normed, decay_down[...])).astype(BF16)
    decay_pre = matmul(decay_low, decay_up[:, own]) + decay_bias[:, own]
    decay = jnp.exp(-math.exp(-0.5) / (1.0 + jnp.exp(-decay_pre)))
    rate_low = matmul_nt(normed, rate_down[...]).astype(BF16)
    rate = 1.0 / (1.0 + jnp.exp(-(matmul(rate_low, rate_up[:, own]) + rate_bias[:, own])))
    part_copy(8).wait()
    recept = matmul(normed, recept_weight[...]).astype(BF16).astype(F32)
    part_copy(9).wait()
    keys = matmul(normed, key_weight[...]).astype(BF16).astype(F32)
    part_copy(10).wait()
    vals = matmul(normed, value_weight[...]).astype(BF16).astype(F32)
    for h in range(heads):
        cols = slice(h * size, (h + 1) * size)
        key_h = keys[:, cols]
        inverse = 1.0 / (jnp.sum(key_h * key_h, axis=-1, keepdims=True) + 1e-06)
        recept_s[:, h, :] = recept[:, cols]
        pull_s[h] = key_h * inverse
        key_rate_s[h] = key_h * rate[:, cols]
        value_s[h] = vals[:, cols]
        decay_s[h] = decay[:, cols]

    shape, flat = (heads, size, size), (heads * size, size)
    eye = lax.broadcasted_iota(jnp.int32, shape, 1) == lax.broadcasted_iota(jnp.int32, shape, 2)
    spread = (heads, width)
    owner = lax.broadcasted_iota(jnp.int32, spread, 0)
    own_lanes = owner == lax.broadcasted_iota(jnp.int32, spread, 1) // size

    def one_sequence(row):
        here = pl.ds(row, 1)
        state = state_v[row]
        gain = jnp.sum(
            jnp.where(eye, value_s[:, here], 0.0) - state * pull_s[:, here], axis=-1, keepdims=True
        )
        new = state * decay_s[:, here] + gain * key_rate_s[:, here]
        new_v[row] = new
        out = matmul_nt(recept_s[row].astype(BF16), new.astype(BF16).reshape(flat))
        readout_s[here, :] = jnp.sum(jnp.where(own_lanes, out, 0.0), axis=0, keepdims=True)

    def one_chunk(c, carry):
        in_copy(c).wait()

        def some(k, inner):
            for j in range(4):
                one_sequence(c * step_rows + k * 4 + j)
            return inner

        lax.fori_loop(0, step_rows // 4, some, 0)
        out_copy(c).start()
        return carry

    lax.fori_loop(0, chunks, one_chunk, 0)

    part_copy(11).wait()
    gain = head_gain[:, own]
    for h in range(heads):
        cols = slice(h * size, (h + 1) * size)
        out = readout_s[:, cols]
        centred = out - jnp.mean(out, axis=-1, keepdims=True)
        variance = jnp.mean(centred * centred, axis=-1, keepdims=True)
        normed_s[:, cols] = (centred * lax.rsqrt(variance + 0.00064) * gain[:, cols]).astype(BF16)
    part_copy(12).wait()
    partial[...] = matmul(normed_s[...], out_weight[...]).astype(BF16)

    def wait_out(c, carry):
        out_copy(c).wait()
        return carry

    lax.fori_loop(0, chunks, wait_out, 0)


def attention(operands, state):
    seqs, heads, size, _ = state.shape
    hidden = operands[0]
    width = heads * size
    chunks = seqs // math.gcd(seqs, 8)
    per_head = pltpu.VMEM((heads, seqs, size), F32)
    dma = pltpu.SemaphoreType.DMA
    any_spec = pl.BlockSpec(memory_space=pl.ANY)
    return pl.pallas_call(
        functools.partial(attention_kernel, chunks),
        out_shape=(
            jax.ShapeDtypeStruct(state.shape, F32),
            jax.ShapeDtypeStruct(hidden.shape, BF16),
        ),
        in_specs=[any_spec] * 14,
        out_specs=(any_spec, VMEM_SPEC),
        scratch_shapes=[pltpu.VMEM(a.shape, a.dtype) for a in operands]
        + [
            pltpu.VMEM(state.shape, F32),
            pltpu.VMEM(state.shape, F32),
            pltpu.VMEM((seqs, heads, size), F32),
            per_head,
            per_head,
            per_head,
            per_head,
            pltpu.VMEM((seqs, width), F32),
            pltpu.VMEM((seqs, width), BF16),
            dma((13,)),
            dma((chunks,)),
            dma((chunks,)),
        ],
        compiler_params=pltpu.CompilerParams(vmem_limit_bytes=VMEM_LIMIT),
        name="attention",
    )(*operands, state)


def position(sizes):
    ep = lax.axis_index("ep")
    strides = (sizes[1] * sizes[2], sizes[2], 1)
    return ep, tuple(ep // s % n for s, n in zip(strides, sizes)), strides


def greet_all(count):
    ep, tp = lax.axis_index("ep"), lax.axis_index("tp")
    barrier = pltpu.get_barrier_semaphore()

    def greet(k, carry):
        pl.semaphore_signal(
            barrier, inc=1, device_id=((ep + k) % count, tp), device_id_type=MESH
        )
        return carry

    lax.fori_loop(1, count, greet, 0)
    pl.semaphore_signal(barrier, inc=1, device_id=(ep, 1 - tp), device_id_type=MESH)
    pl.semaphore_wait(barrier, count)


def remote(src, dst, send, recv, device):
    return pltpu.make_async_remote_copy(
        src_ref=src,
        dst_ref=dst,
        send_sem=send,
        recv_sem=recv,
        device_id=device,
        device_id_type=MESH,
    )


def layer_kernel(
    sizes,
    top,
    cap,
    partial,
    hidden,
    gain,
    blend_vector,
    routing,
    route_scale,
    gate_h,
    up_h,
    down_h,
    expert_gate_h,
    expert_up_h,
    expert_down_h,
    out,
    tokens,
    own_tokens,
    metas,
    meta,
    first,
    sibling_part,
    gate_v,
    up_v,
    down_v,
    expert_gate,
    expert_up,
    expert_down,
    gate_w,
    up_w,
    mix_w,
    mix_rows,
    picked,
    from_sibling,
    lands,
    sems,
):
    (
        weight_sem,
        part_sem,
        meta_sem,
        ag_send,
        ag_recv,
        pass_send,
        pass_recv,
        pair_send,
        pair_recv,
        rs_send,
        rs_recv,
        last_sem,
    ) = sems
    chunks, across, along = sizes
    count = chunks * across * along
    plane = across * along
    ep, at, strides = position(sizes)
    tp = lax.axis_index("tp")
    half, width = first.shape
    seqs = 2 * half
    sibling = (ep, 1 - tp)
    mine = pl.ds(pl.multiple_of(tp * half, half), half)
    other = pl.ds(pl.multiple_of((1 - tp) * half, half), half)
    slots = plane * cap
    depth = gate_w.shape[0]
    units = gate_v.shape[0]
    rows_at_once = max(1, 256 // (along * seqs))
    blocks = across // rows_at_once
    block_chips = rows_at_once * along
    block_rows = block_chips * seqs
    steps = max(sizes[1:]) - 1

    weights = (
        (gate_h, gate_v),
        (up_h, up_v),
        (down_h, down_v),
        (expert_gate_h, expert_gate),
        (expert_up_h, expert_up),
        (expert_down_h, expert_down),
    )

    def weight_copy(i):
        return pltpu.make_async_copy(weights[i][0], weights[i][1], weight_sem.at[i])

    def per_core(run):
        @pl.when(tp == 0)
        def _():
            run(0)

        @pl.when(tp == 1)
        def _():
            run(1)

    def flat(stage, k, j):
        return k if stage == 0 else chunks + ((stage - 1) * chunks + k) * steps + j - 1

    def meta_copy(k):
        peer = (ep + k) % count
        return remote(meta, metas.at[ep], meta_sem.at[0], meta_sem.at[1], (peer, tp))

    gather_orders = ((0, 2, 1), (0, 1, 2))
    scatter_orders = ((1, 2), (2, 1))

    def plane_of(k):
        return (at[0] + chunks - k) % chunks

    def gather_view(core, stage, k, j):
        _, d2, d3 = gather_orders[core]
        spot = [pl.ds(plane_of(k), 1), None, None]

        def one(d, back=0):
            return pl.ds((at[d] + sizes[d] - back) % sizes[d], 1)

        spot[d2] = pl.ds(0, sizes[d2]) if stage == 2 else one(d2, j if stage == 1 else 0)
        spot[d3] = one(d3, j if stage == 2 else 0)
        return tokens.at[tuple(spot) + (pl.ds(core * half, half),)]

    def gather_copy(core, stage, k, j):
        d = gather_orders[core][stage]
        target = gather_view(core, stage, 0 if stage == 0 else k, 0)
        source = own_tokens if stage == 0 else target
        peer = ep + ((at[d] + j) % sizes[d] - at[d]) * strides[d]
        slot = flat(stage, k, j)
        return remote(source, target, ag_send.at[slot], ag_recv.at[slot], (peer, core))

    def pass_on(core, stage, k, j):
        view = gather_view(core, stage, k, j)
        remote(view, view, pass_send.at[k], pass_recv.at[k], sibling).start()

    def plane_pass(core, k):
        view = tokens.at[plane_of(k), :, :, pl.ds(core * half, half)]
        return remote(view, view, pass_send.at[k], pass_recv.at[k], sibling)

    def send_first(core, k):
        if k:
            gather_copy(core, 0, k, k).wait()
        for j in range(1, sizes[gather_orders[core][1]]):
            gather_copy(core, 1, k, j).start()
        pass_on(core, 0, k, 0)

    def send_second(core, k):
        order = gather_orders[core]
        for j in range(1, sizes[order[1]]):
            gather_copy(core, 1, k, j).wait()
        for j in range(1, sizes[order[2]]):
            gather_copy(core, 2, k, j).start()
        for j in range(1, sizes[order[1]]):
            pass_on(core, 1, k, j)

    def plane_done(core, k):
        last = gather_orders[core][2]
        for j in range(1, sizes[last]):
            gather_copy(core, 2, k, j).wait()
        for j in range(1, sizes[last]):
            pass_on(core, 2, k, j)

    def plane_here(core, k):
        plane_pass(core, k).wait_send()
        plane_pass(1 - core, k).wait_recv()

    def select_of(k):
        here = metas[pl.ds(plane_of(k) * plane, plane)]
        lanes = lax.broadcasted_iota(jnp.int32, (plane, 128), 1)
        expert = ep.astype(F32)
        chosen = jnp.zeros((plane, 128), F32)
        scale_of = jnp.zeros((plane, 128), F32)
        for c in range(top):
            hit = jnp.where((here[:, c, :] == expert) & (lanes < seqs), 1.0, 0.0)
            chosen = chosen + hit
            scale_of = scale_of + hit * here[:, top + c, :]
        earlier = lax.broadcasted_iota(jnp.int32, (128, 128), 0) < lax.broadcasted_iota(
            jnp.int32, (128, 128), 1
        )
        rank = matmul(chosen.astype(BF16), jnp.where(earlier, 1.0, 0.0).astype(BF16))
        chip = lax.broadcasted_iota(jnp.int32, (plane, 128), 0).astype(F32)
        return jnp.where(chosen > 0.5, rank + chip * cap, -1.0), scale_of

    def use_tokens(k):
        z = plane_of(k)
        place, scale_of = select_of(k)
        scales = jnp.zeros((slots, 1), F32)
        for i in range(blocks):
            chips = range(i * block_chips, (i + 1) * block_chips)
            place_row = jnp.concatenate([place[p : p + 1, :seqs] for p in chips], axis=1)
            scale_row = jnp.concatenate([scale_of[p : p + 1, :seqs] for p in chips], axis=1)
            slot_of = lax.broadcasted_iota(jnp.int32, (depth, block_rows), 0).astype(F32)
            select = jnp.where(slot_of == place_row, 1.0, 0.0)
            scales = scales + jnp.sum(select[:slots] * scale_row, axis=1, keepdims=True)
            own_slots = slice(i * block_chips * cap, (i + 1) * block_chips * cap)
            own_rows = slice(i * block_rows, (i + 1) * block_rows)
            rows = tokens[z, pl.ds(i * rows_at_once, rows_at_once)].reshape(block_rows, width)
            picked[own_slots, :] = matmul(select[own_slots].astype(BF16), rows).astype(BF16)
            mix_rows[own_rows, :] = jnp.transpose(select).astype(BF16)

        def dense(i, carry):
            rows = tokens[z, pl.ds(i * rows_at_once, rows_at_once)].reshape(block_rows, width)
            gate = matmul_nt(rows, gate_w[...])
            blend = 1.0 / (1.0 + jnp.exp(-gate[:, 0:1]))
            act = silu_of(gate) * matmul_nt(rows, up_w[...]) * blend
            own_rows = pl.ds(pl.multiple_of(i * block_rows, block_rows), block_rows)
            mix_rows[own_rows, :] = (mix_rows[own_rows, :].astype(F32) + act).astype(BF16)
            return carry

        lax.fori_loop(0, blocks, dense, 0)
        return scales

    def run_experts(scales):
        gate = matmul(picked[...], expert_gate[0])
        hidden_rows = (silu_of(gate) * matmul(picked[...], expert_up[0])).astype(BF16)
        mix_w[0:slots, :] = (matmul(hidden_rows, expert_down[0]) * scales).astype(BF16)

    def pair_copy(k):
        return remote(
            tokens.at[plane_of(k), :, :, other],
            from_sibling.at[k],
            pair_send.at[k],
            pair_recv.at[k],
            sibling,
        )

    def make_part(k):
        z = plane_of(k)

        def some(i, carry):
            own_rows = pl.ds(pl.multiple_of(i * block_rows, block_rows), block_rows)
            part = matmul(mix_rows[own_rows, :], mix_w[...]).astype(BF16)
            ys = pl.ds(i * rows_at_once, rows_at_once)
            tokens[z, ys] = part.reshape(rows_at_once, along, seqs, width)
            return carry

        lax.fori_loop(0, blocks, some, 0)
        pair_copy(k).start()

    def spot(core, k, c1, c2):
        d1, d2 = scatter_orders[core]
        place = [plane_of(k), None, None]
        place[d1], place[d2] = c1, c2
        return tuple(place) + (pl.ds(core * half, half),)

    def scatter_copy(core, stage, k, j):
        d1, d2 = scatter_orders[core]
        if stage == 1:
            d = d1
            source = tokens.at[spot(core, k, (at[d1] + j) % sizes[d1], slice(None))]
            target = lands[0].at[k, j - 1]
        elif stage == 2:
            d = d2
            source = tokens.at[spot(core, k, at[d1], (at[d2] + j) % sizes[d2])]
            target = lands[1].at[k, j - 1]
        else:
            d, j = 0, chunks - k
            source = tokens.at[spot(core, k, at[d1], at[d2])]
            target = lands[2].at[k - 1]
        peer = ep + ((at[d] + j) % sizes[d] - at[d]) * strides[d]
        slot = flat(stage, k, j)
        return remote(source, target, rs_send.at[slot], rs_recv.at[slot], (peer, core))

    def pair_sum(k):
        pair_copy(k).wait()
        z = plane_of(k)

        def add(b, carry):
            y, x = b // along, b % along
            tokens[z, y, x, mine, :] = (
                tokens[z, y, x, mine, :].astype(F32) + from_sibling[k, y, x].astype(F32)
            ).astype(BF16)
            return carry

        lax.fori_loop(0, plane, add, 0)

        def send(core):
            for j in range(1, sizes[scatter_orders[core][0]]):
                scatter_copy(core, 1, k, j).start()

        per_core(send)

    def first_sum(core, k):
        d1, d2 = scatter_orders[core]
        for j in range(1, sizes[d1]):
            scatter_copy(core, 1, k, j).wait()

        def add(b, carry):
            place = spot(core, k, at[d1], b)
            value = tokens[place].astype(F32)
            for j in range(1, sizes[d1]):
                value = value + lands[0][k, j - 1, b].astype(F32)
            tokens[place] = value.astype(BF16)
            return carry

        lax.fori_loop(0, sizes[d2], add, 0)
        for j in range(1, sizes[d2]):
            scatter_copy(core, 2, k, j).start()

    def second_sum(core, k):
        d1, d2 = scatter_orders[core]
        for j in range(1, sizes[d2]):
            scatter_copy(core, 2, k, j).wait()
        place = spot(core, k, at[d1], at[d2])
        value = tokens[place].astype(F32)
        for j in range(1, sizes[d2]):
            value = value + lands[1][k, j - 1].astype(F32)
        tokens[place] = value.astype(BF16)
        if k:
            scatter_copy(core, 0, k, 0).start()

    def finish(core):
        value = tokens[spot(core, 0, at[scatter_orders[core][0]], at[scatter_orders[core][1]])]
        value = value.astype(F32) + first[...].astype(F32)
        for k in range(1, chunks):
            scatter_copy(core, 0, k, 0).wait()
            value = value + lands[2][k - 1].astype(F32)
        out[pl.ds(core * half, half), :] = value.astype(BF16)

    for i in range(6):
        weight_copy(i).start()
    meta[...] = jnp.zeros(meta.shape, F32)
    meta[0:top, 0:seqs] = routing[...].astype(F32)
    meta[top : 2 * top, 0:seqs] = route_scale[...]
    base = hidden[mine, :].astype(F32) + partial[mine, :].astype(F32)
    greet_all(count)
    swap = remote(partial.at[other], sibling_part, part_sem.at[0], part_sem.at[1], sibling)
    swap.start()

    def start_meta(k, carry):
        meta_copy(k).start()
        return carry

    lax.fori_loop(1, count, start_meta, 0)
    swap.wait()
    total = (base + sibling_part[...].astype(F32)).astype(BF16)
    first[...] = total
    normed = rms_scaled(total.astype(F32), gain[...]).astype(BF16)
    own_tokens[0, 0, 0] = normed
    tokens[at[0], at[1], at[2], mine, :] = normed

    def start_planes(core):
        send_first(core, 0)
        for k in range(1, chunks):
            gather_copy(core, 0, k, k).start()

    per_core(start_planes)
    metas[ep] = meta[...]
    for i in range(3):
        weight_copy(i).wait()
    blend_row = jnp.concatenate(
        [blend_vector[i : i + 1, :].astype(F32) for i in range(width // 128)], axis=1
    )
    top_row = lax.broadcasted_iota(jnp.int32, (slots, width), 0) == 0
    gate_w[0:slots, :] = jnp.where(top_row, blend_row, 0.0).astype(BF16)
    up_w[0:slots, :] = jnp.zeros((slots, width), BF16)
    if slots + units < depth:
        rest = (depth - slots - units, width)
        gate_w[slots + units : depth, :] = jnp.zeros(rest, BF16)
        up_w[slots + units : depth, :] = jnp.zeros(rest, BF16)
        mix_w[slots + units : depth, :] = jnp.zeros(rest, BF16)
    gate_w[slots : slots + units, :] = gate_v[...]
    up_w[slots : slots + units, :] = up_v[...]
    mix_w[slots : slots + units, :] = down_v[...]

    def at_step(run, k):
        if 0 <= k < chunks:
            per_core(functools.partial(run, k=k))

    for t in range(1, chunks + 4):
        at_step(plane_done, t - 2)
        if 0 <= t - 3 < chunks:
            pair_sum(t - 3)
        at_step(send_second, t - 1)
        if t < chunks:
            at_step(send_first, t)
        at_step(second_sum, t - 4)
        if 0 <= t - 2 < chunks:
            if t == 2:
                some = metas.at[pl.ds(0, count - 1)]
                remote(some, some, meta_sem.at[0], meta_sem.at[1], sibling).wait()
                for i in range(3, 6):
                    weight_copy(i).wait()
            at_step(plane_here, t - 2)
            run_experts(use_tokens(t - 2))
            make_part(t - 2)
        at_step(first_sum, t - 3)
    per_core(finish)

    last = remote(out.at[mine], out.at[mine], last_sem.at[0], last_sem.at[1], sibling)
    last.start()
    last.wait()


def layer_after(sizes, partial, hidden, gain, blend_vector, routing, route_scale, weights):
    seqs, width = hidden.shape
    count = sizes[0] * sizes[1] * sizes[2]
    half, top = seqs // 2, routing.shape[0]
    cap = max(2, 2 * seqs * top // count)
    plane = sizes[1] * sizes[2]
    slots = plane * cap
    depth = -(-(slots + weights[0].shape[0]) // 128) * 128
    chunks, side, block = sizes[0], max(sizes[1:]), (half, width)
    dma = pltpu.SemaphoreType.DMA
    any_spec = pl.BlockSpec(memory_space=pl.ANY)
    hop = dma((chunks * (2 * side - 1),))
    return pl.pallas_call(
        functools.partial(layer_kernel, sizes, top, cap),
        out_shape=jax.ShapeDtypeStruct((seqs, width), BF16),
        in_specs=[VMEM_SPEC] * 6 + [any_spec] * 6,
        out_specs=VMEM_SPEC,
        scratch_shapes=[
            pltpu.VMEM(sizes + (seqs, width), BF16),
            pltpu.VMEM((1, 1, 1) + block, BF16),
            pltpu.VMEM((count, 8, 128), F32),
            pltpu.VMEM((8, 128), F32),
            pltpu.VMEM(block, BF16),
            pltpu.VMEM(block, BF16),
        ]
        + [pltpu.VMEM(w.shape, BF16) for w in weights]
        + [
            pltpu.VMEM((depth, width), BF16),
            pltpu.VMEM((depth, width), BF16),
            pltpu.VMEM((depth, width), BF16),
            pltpu.VMEM((plane * seqs, depth), BF16),
            pltpu.VMEM((slots, width), BF16),
            pltpu.VMEM(sizes + block, BF16),
            [
                pltpu.VMEM((chunks, max(1, side - 1), side) + block, BF16),
                pltpu.VMEM((chunks, max(1, side - 1)) + block, BF16),
                pltpu.VMEM((max(1, chunks - 1),) + block, BF16),
            ],
            [
                dma((6,)),
                dma((2,)),
                dma((2,)),
                hop,
                hop,
                dma((chunks,)),
                dma((chunks,)),
                dma((chunks,)),
                dma((chunks,)),
                hop,
                hop,
                dma((2,)),
            ],
        ],
        compiler_params=pltpu.CompilerParams(
            collective_id=0, has_side_effects=True, vmem_limit_bytes=VMEM_LIMIT
        ),
        name="layer_after",
    )(partial, hidden, gain, blend_vector, routing, route_scale, *weights)


def shards(
    hidden,
    mix_gain,
    recept_weight,
    key_weight,
    value_weight,
    decay_down,
    decay_up,
    decay_bias,
    rate_down,
    rate_up,
    rate_bias,
    head_gain,
    out_weight,
    memory_state,
    ffn_gain,
    blend_vector,
    dense_gate,
    dense_up,
    dense_down,
    expert_gate,
    expert_up,
    expert_down,
    routing,
    route_scale,
):
    sizes = factors_of(lax.axis_size("ep"))
    new_state, partial = attention(
        (
            hidden,
            mix_gain[None],
            decay_down.T,
            rate_down.T,
            decay_up,
            rate_up,
            decay_bias[None],
            rate_bias[None],
            recept_weight,
            key_weight,
            value_weight,
            head_gain[None],
            out_weight,
        ),
        memory_state,
    )
    layer_out = layer_after(
        sizes,
        partial,
        hidden,
        ffn_gain[None],
        blend_vector.reshape(-1, 128),
        routing.T,
        route_scale.T,
        (dense_gate.T, dense_up.T, dense_down, expert_gate, expert_up, expert_down),
    )
    return (layer_out, new_state)


def solution(mesh):
    in_specs = (
        P("ep", None),
        P(),
        P(None, "tp"),
        P(None, "tp"),
        P(None, "tp"),
        P(),
        P(),
        P(),
        P(),
        P(),
        P(),
        P(),
        P("tp", None),
        P("ep", "tp", None, None),
        P(),
        P(),
        P(None, ("ep", "tp")),
        P(None, ("ep", "tp")),
        P(("ep", "tp"), None),
        P("ep", None, "tp"),
        P("ep", None, "tp"),
        P("ep", "tp", None),
        P("ep", None),
        P("ep", None),
    )
    out_specs = (P("ep", None), P("ep", "tp", None, None))
    return jax.shard_map(shards, mesh=mesh, in_specs=in_specs, out_specs=out_specs, check_vma=False)
```

```python
import functools
import math

import jax
import jax.numpy as jnp
from jax import lax
from jax.experimental import pallas as pl
from jax.experimental.pallas import tpu as pltpu
from jax.sharding import PartitionSpec as P

MESH = pl.DeviceIdType.MESH
F32 = jnp.float32
BF16 = jnp.bfloat16
VMEM_LIMIT = 64 * 1024 * 1024 - 65536
VMEM_SPEC = pl.BlockSpec(memory_space=pltpu.VMEM)


def matmul(left, right):
    return jnp.dot(left, right, preferred_element_type=F32)


def matmul_nt(left, right):
    return lax.dot_general(left, right, (((1,), (1,)), ((), ())), preferred_element_type=F32)


def silu_of(tensor):
    return tensor / (1.0 + jnp.exp(-tensor))


def rms_scaled(values, gain):
    return values * lax.rsqrt(jnp.mean(values * values, axis=-1, keepdims=True) + 1e-06) * gain


def factors_of(count):
    slow = 4 if count % 4 == 0 else 1
    rest = count // slow
    mid = math.isqrt(rest)
    while rest % mid:
        mid -= 1
    return slow, mid, rest // mid


def attention_kernel(chunks, *refs):
    sources, (state_h, state_out_h, partial), rest = refs[:13], refs[13:16], refs[16:]
    local, rest = rest[:13], rest[13:]
    state_v, new_v, recept_s, pull_s, key_rate_s, value_s, decay_s, readout_s, normed_s = rest[:9]
    part_sem, in_sem, out_sem = rest[9:]
    (
        hidden,
        mix_gain,
        decay_down,
        rate_down,
        decay_up,
        rate_up,
        decay_bias,
        rate_bias,
        recept_weight,
        key_weight,
        value_weight,
        head_gain,
        out_weight,
    ) = local
    heads, seqs, size = pull_s.shape
    width = heads * size
    step_rows = seqs // chunks
    own = pl.ds(pl.multiple_of(lax.axis_index("tp") * width, 128), width)

    def part_copy(i):
        return pltpu.make_async_copy(sources[i], local[i], part_sem.at[i])

    def rows_of(c):
        return pl.ds(c * step_rows, step_rows)

    def in_copy(c):
        return pltpu.make_async_copy(state_h.at[rows_of(c)], state_v.at[rows_of(c)], in_sem.at[c])

    def out_copy(c):
        return pltpu.make_async_copy(new_v.at[rows_of(c)], state_out_h.at[rows_of(c)], out_sem.at[c])

    for i in range(11):
        part_copy(i).start()

    def start_in(c, carry):
        in_copy(c).start()
        return carry

    lax.fori_loop(0, chunks, start_in, 0)
    part_copy(11).start()
    part_copy(12).start()

    part_copy(0).wait()
    part_copy(1).wait()
    normed = rms_scaled(hidden[...].astype(F32), mix_gain[...]).astype(BF16)
    for i in range(2, 8):
        part_copy(i).wait()
    decay_low = jnp.tanh(matmul_nt(normed, decay_down[...])).astype(BF16)
    decay_pre = matmul(decay_low, decay_up[:, own]) + decay_bias[:, own]
    decay = jnp.exp(-math.exp(-0.5) / (1.0 + jnp.exp(-decay_pre)))
    rate_low = matmul_nt(normed, rate_down[...]).astype(BF16)
    rate = 1.0 / (1.0 + jnp.exp(-(matmul(rate_low, rate_up[:, own]) + rate_bias[:, own])))
    part_copy(8).wait()
    recept = matmul(normed, recept_weight[...]).astype(BF16).astype(F32)
    part_copy(9).wait()
    keys = matmul(normed, key_weight[...]).astype(BF16).astype(F32)
    part_copy(10).wait()
    vals = matmul(normed, value_weight[...]).astype(BF16).astype(F32)
    for h in range(heads):
        cols = slice(h * size, (h + 1) * size)
        key_h = keys[:, cols]
        inverse = 1.0 / (jnp.sum(key_h * key_h, axis=-1, keepdims=True) + 1e-06)
        recept_s[:, h, :] = recept[:, cols]
        pull_s[h] = key_h * inverse
        key_rate_s[h] = key_h * rate[:, cols]
        value_s[h] = vals[:, cols]
        decay_s[h] = decay[:, cols]

    shape, flat = (heads, size, size), (heads * size, size)
    eye = lax.broadcasted_iota(jnp.int32, shape, 1) == lax.broadcasted_iota(jnp.int32, shape, 2)
    spread = (heads, width)
    owner = lax.broadcasted_iota(jnp.int32, spread, 0)
    own_lanes = owner == lax.broadcasted_iota(jnp.int32, spread, 1) // size

    def one_sequence(row):
        here = pl.ds(row, 1)
        state = state_v[row]
        gain = jnp.sum(
            jnp.where(eye, value_s[:, here], 0.0) - state * pull_s[:, here], axis=-1, keepdims=True
        )
        new = state * decay_s[:, here] + gain * key_rate_s[:, here]
        new_v[row] = new
        out = matmul_nt(recept_s[row].astype(BF16), new.astype(BF16).reshape(flat))
        readout_s[here, :] = jnp.sum(jnp.where(own_lanes, out, 0.0), axis=0, keepdims=True)

    def one_chunk(c, carry):
        in_copy(c).wait()

        def some(k, inner):
            for j in range(4):
                one_sequence(c * step_rows + k * 4 + j)
            return inner

        lax.fori_loop(0, step_rows // 4, some, 0)
        out_copy(c).start()
        return carry

    lax.fori_loop(0, chunks, one_chunk, 0)

    part_copy(11).wait()
    gain = head_gain[:, own]
    for h in range(heads):
        cols = slice(h * size, (h + 1) * size)
        out = readout_s[:, cols]
        centred = out - jnp.mean(out, axis=-1, keepdims=True)
        variance = jnp.mean(centred * centred, axis=-1, keepdims=True)
        normed_s[:, cols] = (centred * lax.rsqrt(variance + 0.00064) * gain[:, cols]).astype(BF16)
    part_copy(12).wait()
    partial[...] = matmul(normed_s[...], out_weight[...]).astype(BF16)

    def wait_out(c, carry):
        out_copy(c).wait()
        return carry

    lax.fori_loop(0, chunks, wait_out, 0)


def attention(operands, state):
    seqs, heads, size, _ = state.shape
    hidden = operands[0]
    width = heads * size
    chunks = seqs // math.gcd(seqs, 8)
    per_head = pltpu.VMEM((heads, seqs, size), F32)
    dma = pltpu.SemaphoreType.DMA
    any_spec = pl.BlockSpec(memory_space=pl.ANY)
    return pl.pallas_call(
        functools.partial(attention_kernel, chunks),
        out_shape=(
            jax.ShapeDtypeStruct(state.shape, F32),
            jax.ShapeDtypeStruct(hidden.shape, BF16),
        ),
        in_specs=[any_spec] * 14,
        out_specs=(any_spec, VMEM_SPEC),
        scratch_shapes=[pltpu.VMEM(a.shape, a.dtype) for a in operands]
        + [
            pltpu.VMEM(state.shape, F32),
            pltpu.VMEM(state.shape, F32),
            pltpu.VMEM((seqs, heads, size), F32),
            per_head,
            per_head,
            per_head,
            per_head,
            pltpu.VMEM((seqs, width), F32),
            pltpu.VMEM((seqs, width), BF16),
            dma((13,)),
            dma((chunks,)),
            dma((chunks,)),
        ],
        compiler_params=pltpu.CompilerParams(vmem_limit_bytes=VMEM_LIMIT),
        name="attention",
    )(*operands, state)


def position(sizes):
    ep = lax.axis_index("ep")
    strides = (sizes[1] * sizes[2], sizes[2], 1)
    return ep, tuple(ep // s % n for s, n in zip(strides, sizes)), strides


def greet_all(count):
    ep, tp = lax.axis_index("ep"), lax.axis_index("tp")
    barrier = pltpu.get_barrier_semaphore()

    def greet(k, carry):
        pl.semaphore_signal(
            barrier, inc=1, device_id=((ep + k) % count, tp), device_id_type=MESH
        )
        return carry

    lax.fori_loop(1, count, greet, 0)
    pl.semaphore_signal(barrier, inc=1, device_id=(ep, 1 - tp), device_id_type=MESH)
    pl.semaphore_wait(barrier, count)


def remote(src, dst, send, recv, device):
    return pltpu.make_async_remote_copy(
        src_ref=src,
        dst_ref=dst,
        send_sem=send,
        recv_sem=recv,
        device_id=device,
        device_id_type=MESH,
    )


def layer_kernel(
    sizes,
    top,
    cap,
    partial,
    hidden,
    gain,
    blend_vector,
    routing,
    route_scale,
    gate_h,
    up_h,
    down_h,
    expert_gate_h,
    expert_up_h,
    expert_down_h,
    out,
    tokens,
    own_tokens,
    metas,
    meta,
    first,
    sibling_part,
    gate_v,
    up_v,
    down_v,
    expert_gate,
    expert_up,
    expert_down,
    gate_w,
    up_w,
    mix_w,
    mix_rows,
    picked,
    from_sibling,
    lands,
    sems,
):
    (
        weight_sem,
        part_sem,
        meta_sem,
        ag_send,
        ag_recv,
        pass_send,
        pass_recv,
        pair_send,
        pair_recv,
        rs_send,
        rs_recv,
        last_sem,
    ) = sems
    chunks, across, along = sizes
    count = chunks * across * along
    plane = across * along
    ep, at, strides = position(sizes)
    tp = lax.axis_index("tp")
    half, width = first.shape
    seqs = 2 * half
    sibling = (ep, 1 - tp)
    mine = pl.ds(pl.multiple_of(tp * half, half), half)
    other = pl.ds(pl.multiple_of((1 - tp) * half, half), half)
    slots = plane * cap
    depth = gate_w.shape[0]
    units = gate_v.shape[0]
    rows_at_once = max(1, 256 // (along * seqs))
    blocks = across // rows_at_once
    block_chips = rows_at_once * along
    block_rows = block_chips * seqs
    steps = max(sizes[1:]) - 1

    weights = (
        (gate_h, gate_v),
        (up_h, up_v),
        (down_h, down_v),
        (expert_gate_h, expert_gate),
        (expert_up_h, expert_up),
        (expert_down_h, expert_down),
    )

    def weight_copy(i):
        return pltpu.make_async_copy(weights[i][0], weights[i][1], weight_sem.at[i])

    def per_core(run):
        @pl.when(tp == 0)
        def _():
            run(0)

        @pl.when(tp == 1)
        def _():
            run(1)

    def one_slot(k, j):
        return chunks + k * steps + j - 1

    def two_slot(k, j, i):
        return chunks * (1 + steps) + (k * steps + j - 1) * (steps + 1) + i

    def meta_copy(k):
        peer = (ep + k) % count
        return remote(meta, metas.at[ep], meta_sem.at[0], meta_sem.at[1], (peer, tp))

    gather_orders = ((0, 2, 1), (0, 1, 2))
    scatter_orders = ((1, 2), (2, 1))

    def plane_of(k):
        return (at[0] + chunks - k) % chunks

    def gather_view(core, k, i, j):
        _, d2, d3 = gather_orders[core]
        spot = [pl.ds(plane_of(k), 1), None, None]

        def one(d, back):
            return pl.ds((at[d] + sizes[d] - back) % sizes[d], 1)

        spot[d2] = pl.ds(0, sizes[d2]) if i is None else one(d2, i)
        spot[d3] = one(d3, j)
        return tokens.at[tuple(spot) + (pl.ds(core * half, half),)]

    def peer_of(d, j):
        return ep + ((at[d] + j) % sizes[d] - at[d]) * strides[d]

    def gather_copy(core, stage, k, j, i=0):
        target = gather_view(core, 0 if stage == 0 else k, i, 0)
        source = own_tokens if stage == 0 else target
        slot = (k, one_slot(k, j), two_slot(k, j, i))[stage]
        peer = peer_of(gather_orders[core][stage], j)
        return remote(source, target, ag_send.at[slot], ag_recv.at[slot], (peer, core))

    def pass_on(core, k, i, j):
        view = gather_view(core, k, i, j)
        remote(view, view, pass_send.at[k], pass_recv.at[k], sibling).start()

    def plane_pass(core, k):
        view = tokens.at[plane_of(k), :, :, pl.ds(core * half, half)]
        return remote(view, view, pass_send.at[k], pass_recv.at[k], sibling)

    def send_first(core, k):
        order = gather_orders[core]
        if k:
            gather_copy(core, 0, k, k).wait()
        for j in range(1, sizes[order[1]]):
            gather_copy(core, 1, k, j).start()
        for j in range(1, sizes[order[2]]):
            gather_copy(core, 2, k, j, 0).start()
        pass_on(core, k, 0, 0)

    def send_second(core, k):
        order = gather_orders[core]
        for i in range(1, sizes[order[1]]):
            gather_copy(core, 1, k, i).wait()
            for j in range(1, sizes[order[2]]):
                gather_copy(core, 2, k, j, i).start()
            pass_on(core, k, i, 0)

    def plane_done(core, k):
        order = gather_orders[core]
        for j in range(1, sizes[order[2]]):
            for i in range(sizes[order[1]]):
                gather_copy(core, 2, k, j, i).wait()
            pass_on(core, k, None, j)

    def plane_here(core, k):
        plane_pass(core, k).wait_send()
        plane_pass(1 - core, k).wait_recv()

    def select_of(k):
        here = metas[pl.ds(plane_of(k) * plane, plane)]
        lanes = lax.broadcasted_iota(jnp.int32, (plane, 128), 1)
        expert = ep.astype(F32)
        chosen = jnp.zeros((plane, 128), F32)
        scale_of = jnp.zeros((plane, 128), F32)
        for c in range(top):
            hit = jnp.where((here[:, c, :] == expert) & (lanes < seqs), 1.0, 0.0)
            chosen = chosen + hit
            scale_of = scale_of + hit * here[:, top + c, :]
        earlier = lax.broadcasted_iota(jnp.int32, (128, 128), 0) < lax.broadcasted_iota(
            jnp.int32, (128, 128), 1
        )
        rank = matmul(chosen.astype(BF16), jnp.where(earlier, 1.0, 0.0).astype(BF16))
        chip = lax.broadcasted_iota(jnp.int32, (plane, 128), 0).astype(F32)
        return jnp.where(chosen > 0.5, rank + chip * cap, -1.0), scale_of

    def use_tokens(k):
        z = plane_of(k)
        place, scale_of = select_of(k)
        scales = jnp.zeros((slots, 1), F32)
        for i in range(blocks):
            chips = range(i * block_chips, (i + 1) * block_chips)
            place_row = jnp.concatenate([place[p : p + 1, :seqs] for p in chips], axis=1)
            scale_row = jnp.concatenate([scale_of[p : p + 1, :seqs] for p in chips], axis=1)
            slot_of = lax.broadcasted_iota(jnp.int32, (depth, block_rows), 0).astype(F32)
            select = jnp.where(slot_of == place_row, 1.0, 0.0)
            scales = scales + jnp.sum(select[:slots] * scale_row, axis=1, keepdims=True)
            own_slots = slice(i * block_chips * cap, (i + 1) * block_chips * cap)
            own_rows = slice(i * block_rows, (i + 1) * block_rows)
            rows = tokens[z, pl.ds(i * rows_at_once, rows_at_once)].reshape(block_rows, width)
            picked[own_slots, :] = matmul(select[own_slots].astype(BF16), rows).astype(BF16)
            mix_rows[0, own_rows, :] = jnp.transpose(select).astype(BF16)

        def dense(i, carry):
            rows = tokens[z, pl.ds(i * rows_at_once, rows_at_once)].reshape(block_rows, width)
            gate = matmul_nt(rows, gate_w[...])
            blend = 1.0 / (1.0 + jnp.exp(-gate[:, 0:1]))
            act = silu_of(gate) * matmul_nt(rows, up_w[...]) * blend
            own_rows = pl.ds(pl.multiple_of(i * block_rows, block_rows), block_rows)
            routed = mix_rows[0, own_rows, :].astype(F32)
            mix_rows[0, own_rows, :] = (routed + act).astype(BF16)
            return carry

        lax.fori_loop(0, blocks, dense, 0)
        return scales

    def run_experts(k, scales):
        gate = matmul(picked[...], expert_gate[0])
        hidden_rows = (silu_of(gate) * matmul(picked[...], expert_up[0])).astype(BF16)
        mix_w[0, 0:slots, :] = (matmul(hidden_rows, expert_down[0]) * scales).astype(BF16)

    def pair_copy(k):
        return remote(
            tokens.at[plane_of(k), :, :, other],
            from_sibling.at[k],
            pair_send.at[k],
            pair_recv.at[k],
            sibling,
        )

    def make_part(k):
        z = plane_of(k)

        def some(i, carry):
            own_rows = pl.ds(pl.multiple_of(i * block_rows, block_rows), block_rows)
            part = matmul(mix_rows[0, own_rows, :], mix_w[0]).astype(BF16)
            ys = pl.ds(i * rows_at_once, rows_at_once)
            tokens[z, ys] = part.reshape(rows_at_once, along, seqs, width)
            return carry

        lax.fori_loop(0, blocks, some, 0)
        pair_copy(k).start()

    def spot(core, k, j=0, i=0):
        d1, d2 = scatter_orders[core]
        place = [plane_of(k), None, None]
        place[d1], place[d2] = (at[d1] + j) % sizes[d1], (at[d2] + i) % sizes[d2]
        return tuple(place) + (pl.ds(core * half, half),)

    def scatter_copy(core, stage, k, j=0, i=0):
        d1, d2 = scatter_orders[core]
        if stage == 0:
            peer, slot, target = peer_of(0, chunks - k), k, lands[2].at[k - 1]
        elif stage == 1:
            peer, slot, target = peer_of(d1, j), two_slot(k, j, i), lands[0].at[k, j - 1, i]
        else:
            peer, slot, target = peer_of(d2, i), one_slot(k, i), lands[1].at[k, i - 1]
        source = tokens.at[spot(core, k, j, i)]
        return remote(source, target, rs_send.at[slot], rs_recv.at[slot], (peer, core))

    def pair_sum(k):
        pair_copy(k).wait()
        z = plane_of(k)

        def add(b, carry):
            y, x = b // along, b % along
            tokens[z, y, x, mine, :] = (
                tokens[z, y, x, mine, :].astype(F32) + from_sibling[k, y, x].astype(F32)
            ).astype(BF16)
            return carry

        lax.fori_loop(0, plane, add, 0)

        def send(core):
            d1, d2 = scatter_orders[core]
            for i in range(sizes[d2] - 1, -1, -1):
                for j in range(1, sizes[d1]):
                    scatter_copy(core, 1, k, j, i).start()

        per_core(send)

    def first_sum(core, k):
        d1, d2 = scatter_orders[core]
        for i in range(sizes[d2] - 1, 0, -1):
            place = spot(core, k, 0, i)
            value = tokens[place].astype(F32)
            for j in range(1, sizes[d1]):
                scatter_copy(core, 1, k, j, i).wait()
                value = value + lands[0][k, j - 1, i].astype(F32)
            tokens[place] = value.astype(BF16)
            scatter_copy(core, 2, k, 0, i).start()

    def second_sum(core, k):
        d1, d2 = scatter_orders[core]
        place = spot(core, k)
        value = tokens[place].astype(F32)
        for j in range(1, sizes[d1]):
            scatter_copy(core, 1, k, j, 0).wait()
            value = value + lands[0][k, j - 1, 0].astype(F32)
        for i in range(1, sizes[d2]):
            scatter_copy(core, 2, k, 0, i).wait()
            value = value + lands[1][k, i - 1].astype(F32)
        tokens[place] = value.astype(BF16)
        if k:
            scatter_copy(core, 0, k).start()

    def finish(core):
        value = tokens[spot(core, 0)].astype(F32) + first[...].astype(F32)
        for k in range(1, chunks):
            scatter_copy(core, 0, k).wait()
            value = value + lands[2][k - 1].astype(F32)
        out[pl.ds(core * half, half), :] = value.astype(BF16)

    for i in range(6):
        weight_copy(i).start()
    meta[...] = jnp.zeros(meta.shape, F32)
    meta[0:top, 0:seqs] = routing[...].astype(F32)
    meta[top : 2 * top, 0:seqs] = route_scale[...]
    base = hidden[mine, :].astype(F32) + partial[mine, :].astype(F32)
    greet_all(count)
    swap = remote(partial.at[other], sibling_part, part_sem.at[0], part_sem.at[1], sibling)
    swap.start()

    def start_meta(k, carry):
        meta_copy(k).start()
        return carry

    lax.fori_loop(1, count, start_meta, 0)
    swap.wait()
    total = (base + sibling_part[...].astype(F32)).astype(BF16)
    first[...] = total
    normed = rms_scaled(total.astype(F32), gain[...]).astype(BF16)
    own_tokens[0, 0, 0] = normed
    tokens[at[0], at[1], at[2], mine, :] = normed

    def start_planes(core):
        send_first(core, 0)
        for k in range(1, chunks):
            gather_copy(core, 0, k, k).start()

    per_core(start_planes)
    metas[ep] = meta[...]
    for i in range(3):
        weight_copy(i).wait()
    blend_row = jnp.concatenate(
        [blend_vector[i : i + 1, :].astype(F32) for i in range(width // 128)], axis=1
    )
    top_row = lax.broadcasted_iota(jnp.int32, (slots, width), 0) == 0
    gate_w[0:slots, :] = jnp.where(top_row, blend_row, 0.0).astype(BF16)
    up_w[0:slots, :] = jnp.zeros((slots, width), BF16)
    if slots + units < depth:
        rest = (depth - slots - units, width)
        gate_w[slots + units : depth, :] = jnp.zeros(rest, BF16)
        up_w[slots + units : depth, :] = jnp.zeros(rest, BF16)
        for b in range(2):
            mix_w[b, slots + units : depth, :] = jnp.zeros(rest, BF16)
    gate_w[slots : slots + units, :] = gate_v[...]
    up_w[slots : slots + units, :] = up_v[...]
    for b in range(2):
        mix_w[b, slots : slots + units, :] = down_v[...]

    def on_core(run, k):
        if 0 <= k < chunks:
            per_core(functools.partial(run, k=k))

    def pair_step(k):
        if 0 <= k < chunks:
            pair_sum(k)

    on_core(send_second, 0)
    on_core(send_first, 1)
    on_core(send_second, 1)
    on_core(plane_done, 0)
    on_core(send_first, 2)
    some = metas.at[pl.ds(0, count - 1)]
    remote(some, some, meta_sem.at[0], meta_sem.at[1], sibling).wait()
    for i in range(3, 6):
        weight_copy(i).wait()
    on_core(plane_here, 0)
    scales = use_tokens(0)
    on_core(send_second, 2)
    on_core(send_first, 3)
    on_core(plane_done, 1)
    run_experts(0, scales)
    make_part(0)
    for k in range(1, chunks):
        on_core(plane_here, k)
        scales = use_tokens(k)
        on_core(send_second, k + 2)
        on_core(send_first, k + 3)
        pair_sum(k - 1)
        if k > 2:
            on_core(first_sum, k - 2)
        run_experts(k, scales)
        on_core(plane_done, k + 1)
        make_part(k)
        if k == 2:
            on_core(first_sum, 0)
    on_core(first_sum, chunks - 2) if chunks > 2 else None
    pair_sum(chunks - 1)
    if chunks == 2:
        on_core(first_sum, 0)
    on_core(second_sum, chunks - 4)
    on_core(second_sum, chunks - 3)
    on_core(second_sum, chunks - 2)
    on_core(first_sum, chunks - 1)
    on_core(second_sum, chunks - 1)
    per_core(finish)

    last = remote(out.at[mine], out.at[mine], last_sem.at[0], last_sem.at[1], sibling)
    last.start()
    last.wait()


def layer_after(sizes, partial, hidden, gain, blend_vector, routing, route_scale, weights):
    seqs, width = hidden.shape
    count = sizes[0] * sizes[1] * sizes[2]
    half, top = seqs // 2, routing.shape[0]
    cap = max(2, 2 * seqs * top // count)
    plane = sizes[1] * sizes[2]
    slots = plane * cap
    depth = -(-(slots + weights[0].shape[0]) // 128) * 128
    chunks, side, block = sizes[0], max(sizes[1:]), (half, width)
    dma = pltpu.SemaphoreType.DMA
    any_spec = pl.BlockSpec(memory_space=pl.ANY)
    hop = dma((chunks * (side * side),))
    return pl.pallas_call(
        functools.partial(layer_kernel, sizes, top, cap),
        out_shape=jax.ShapeDtypeStruct((seqs, width), BF16),
        in_specs=[VMEM_SPEC] * 6 + [any_spec] * 6,
        out_specs=VMEM_SPEC,
        scratch_shapes=[
            pltpu.VMEM(sizes + (seqs, width), BF16),
            pltpu.VMEM((1, 1, 1) + block, BF16),
            pltpu.VMEM((count, 8, 128), F32),
            pltpu.VMEM((8, 128), F32),
            pltpu.VMEM(block, BF16),
            pltpu.VMEM(block, BF16),
        ]
        + [pltpu.VMEM(w.shape, BF16) for w in weights]
        + [
            pltpu.VMEM((depth, width), BF16),
            pltpu.VMEM((depth, width), BF16),
            pltpu.VMEM((2, depth, width), BF16),
            pltpu.VMEM((2, plane * seqs, depth), BF16),
            pltpu.VMEM((slots, width), BF16),
            pltpu.VMEM(sizes + block, BF16),
            [
                pltpu.VMEM((chunks, max(1, side - 1), side) + block, BF16),
                pltpu.VMEM((chunks, max(1, side - 1)) + block, BF16),
                pltpu.VMEM((max(1, chunks - 1),) + block, BF16),
            ],
            [
                dma((6,)),
                dma((2,)),
                dma((2,)),
                hop,
                hop,
                dma((chunks,)),
                dma((chunks,)),
                dma((chunks,)),
                dma((chunks,)),
                hop,
                hop,
                dma((2,)),
            ],
        ],
        compiler_params=pltpu.CompilerParams(
            collective_id=0, has_side_effects=True, vmem_limit_bytes=VMEM_LIMIT
        ),
        name="layer_after",
    )(partial, hidden, gain, blend_vector, routing, route_scale, *weights)


def shards(
    hidden,
    mix_gain,
    recept_weight,
    key_weight,
    value_weight,
    decay_down,
    decay_up,
    decay_bias,
    rate_down,
    rate_up,
    rate_bias,
    head_gain,
    out_weight,
    memory_state,
    ffn_gain,
    blend_vector,
    dense_gate,
    dense_up,
    dense_down,
    expert_gate,
    expert_up,
    expert_down,
    routing,
    route_scale,
):
    sizes = factors_of(lax.axis_size("ep"))
    new_state, partial = attention(
        (
            hidden,
            mix_gain[None],
            decay_down.T,
            rate_down.T,
            decay_up,
            rate_up,
            decay_bias[None],
            rate_bias[None],
            recept_weight,
            key_weight,
            value_weight,
            head_gain[None],
            out_weight,
        ),
        memory_state,
    )
    layer_out = layer_after(
        sizes,
        partial,
        hidden,
        ffn_gain[None],
        blend_vector.reshape(-1, 128),
        routing.T,
        route_scale.T,
        (dense_gate.T, dense_up.T, dense_down, expert_gate, expert_up, expert_down),
    )
    return (layer_out, new_state)


def solution(mesh):
    in_specs = (
        P("ep", None),
        P(),
        P(None, "tp"),
        P(None, "tp"),
        P(None, "tp"),
        P(),
        P(),
        P(),
        P(),
        P(),
        P(),
        P(),
        P("tp", None),
        P("ep", "tp", None, None),
        P(),
        P(),
        P(None, ("ep", "tp")),
        P(None, ("ep", "tp")),
        P(("ep", "tp"), None),
        P("ep", None, "tp"),
        P("ep", None, "tp"),
        P("ep", "tp", None),
        P("ep", None),
        P("ep", None),
    )
    out_specs = (P("ep", None), P("ep", "tp", None, None))
    return jax.shard_map(shards, mesh=mesh, in_specs=in_specs, out_specs=out_specs, check_vma=False)
```

```python
import functools
import math

import jax
import jax.numpy as jnp
from jax import lax
from jax.experimental import pallas as pl
from jax.experimental.pallas import tpu as pltpu
from jax.sharding import PartitionSpec as P

MESH = pl.DeviceIdType.MESH
F32 = jnp.float32
BF16 = jnp.bfloat16
VMEM_LIMIT = 64 * 1024 * 1024 - 65536
VMEM_SPEC = pl.BlockSpec(memory_space=pltpu.VMEM)


def matmul(left, right):
    return jnp.dot(left, right, preferred_element_type=F32)


def matmul_nt(left, right):
    return lax.dot_general(left, right, (((1,), (1,)), ((), ())), preferred_element_type=F32)


def silu_of(tensor):
    return tensor / (1.0 + jnp.exp(-tensor))


def rms_scaled(values, gain):
    return values * lax.rsqrt(jnp.mean(values * values, axis=-1, keepdims=True) + 1e-06) * gain


def factors_of(count):
    slow = 4 if count % 4 == 0 else 1
    rest = count // slow
    mid = math.isqrt(rest)
    while rest % mid:
        mid -= 1
    return slow, mid, rest // mid


def attention_kernel(chunks, *refs):
    sources, (state_h, state_out_h, partial), rest = refs[:13], refs[13:16], refs[16:]
    local, rest = rest[:13], rest[13:]
    state_v, new_v, recept_s, pull_s, key_rate_s, value_s, decay_s, readout_s, normed_s = rest[:9]
    part_sem, in_sem, out_sem = rest[9:]
    (
        hidden,
        mix_gain,
        decay_down,
        rate_down,
        decay_up,
        rate_up,
        decay_bias,
        rate_bias,
        recept_weight,
        key_weight,
        value_weight,
        head_gain,
        out_weight,
    ) = local
    heads, seqs, size = pull_s.shape
    width = heads * size
    step_rows = seqs // chunks
    own = pl.ds(pl.multiple_of(lax.axis_index("tp") * width, 128), width)

    def part_copy(i):
        return pltpu.make_async_copy(sources[i], local[i], part_sem.at[i])

    def rows_of(c):
        return pl.ds(c * step_rows, step_rows)

    def in_copy(c):
        return pltpu.make_async_copy(state_h.at[rows_of(c)], state_v.at[rows_of(c)], in_sem.at[c])

    def out_copy(c):
        return pltpu.make_async_copy(new_v.at[rows_of(c)], state_out_h.at[rows_of(c)], out_sem.at[c])

    for i in range(11):
        part_copy(i).start()

    def start_in(c, carry):
        in_copy(c).start()
        return carry

    lax.fori_loop(0, chunks, start_in, 0)
    part_copy(11).start()
    part_copy(12).start()

    part_copy(0).wait()
    part_copy(1).wait()
    normed = rms_scaled(hidden[...].astype(F32), mix_gain[...]).astype(BF16)
    for i in range(2, 8):
        part_copy(i).wait()
    decay_low = jnp.tanh(matmul_nt(normed, decay_down[...])).astype(BF16)
    decay_pre = matmul(decay_low, decay_up[:, own]) + decay_bias[:, own]
    decay = jnp.exp(-math.exp(-0.5) / (1.0 + jnp.exp(-decay_pre)))
    rate_low = matmul_nt(normed, rate_down[...]).astype(BF16)
    rate = 1.0 / (1.0 + jnp.exp(-(matmul(rate_low, rate_up[:, own]) + rate_bias[:, own])))
    part_copy(8).wait()
    recept = matmul(normed, recept_weight[...]).astype(BF16).astype(F32)
    part_copy(9).wait()
    keys = matmul(normed, key_weight[...]).astype(BF16).astype(F32)
    part_copy(10).wait()
    vals = matmul(normed, value_weight[...]).astype(BF16).astype(F32)
    for h in range(heads):
        cols = slice(h * size, (h + 1) * size)
        key_h = keys[:, cols]
        inverse = 1.0 / (jnp.sum(key_h * key_h, axis=-1, keepdims=True) + 1e-06)
        recept_s[:, h, :] = recept[:, cols]
        pull_s[h] = key_h * inverse
        key_rate_s[h] = key_h * rate[:, cols]
        value_s[h] = vals[:, cols]
        decay_s[h] = decay[:, cols]

    shape, flat = (heads, size, size), (heads * size, size)
    eye = lax.broadcasted_iota(jnp.int32, shape, 1) == lax.broadcasted_iota(jnp.int32, shape, 2)
    spread = (heads, width)
    owner = lax.broadcasted_iota(jnp.int32, spread, 0)
    own_lanes = owner == lax.broadcasted_iota(jnp.int32, spread, 1) // size

    def one_sequence(row):
        here = pl.ds(row, 1)
        state = state_v[row]
        gain = jnp.sum(
            jnp.where(eye, value_s[:, here], 0.0) - state * pull_s[:, here], axis=-1, keepdims=True
        )
        new = state * decay_s[:, here] + gain * key_rate_s[:, here]
        new_v[row] = new
        out = matmul_nt(recept_s[row].astype(BF16), new.astype(BF16).reshape(flat))
        readout_s[here, :] = jnp.sum(jnp.where(own_lanes, out, 0.0), axis=0, keepdims=True)

    def one_chunk(c, carry):
        in_copy(c).wait()

        def some(k, inner):
            for j in range(4):
                one_sequence(c * step_rows + k * 4 + j)
            return inner

        lax.fori_loop(0, step_rows // 4, some, 0)
        out_copy(c).start()
        return carry

    lax.fori_loop(0, chunks, one_chunk, 0)

    part_copy(11).wait()
    gain = head_gain[:, own]
    for h in range(heads):
        cols = slice(h * size, (h + 1) * size)
        out = readout_s[:, cols]
        centred = out - jnp.mean(out, axis=-1, keepdims=True)
        variance = jnp.mean(centred * centred, axis=-1, keepdims=True)
        normed_s[:, cols] = (centred * lax.rsqrt(variance + 0.00064) * gain[:, cols]).astype(BF16)
    part_copy(12).wait()
    partial[...] = matmul(normed_s[...], out_weight[...]).astype(BF16)

    def wait_out(c, carry):
        out_copy(c).wait()
        return carry

    lax.fori_loop(0, chunks, wait_out, 0)


def attention(operands, state):
    seqs, heads, size, _ = state.shape
    hidden = operands[0]
    width = heads * size
    chunks = seqs // math.gcd(seqs, 8)
    per_head = pltpu.VMEM((heads, seqs, size), F32)
    dma = pltpu.SemaphoreType.DMA
    any_spec = pl.BlockSpec(memory_space=pl.ANY)
    return pl.pallas_call(
        functools.partial(attention_kernel, chunks),
        out_shape=(
            jax.ShapeDtypeStruct(state.shape, F32),
            jax.ShapeDtypeStruct(hidden.shape, BF16),
        ),
        in_specs=[any_spec] * 14,
        out_specs=(any_spec, VMEM_SPEC),
        scratch_shapes=[pltpu.VMEM(a.shape, a.dtype) for a in operands]
        + [
            pltpu.VMEM(state.shape, F32),
            pltpu.VMEM(state.shape, F32),
            pltpu.VMEM((seqs, heads, size), F32),
            per_head,
            per_head,
            per_head,
            per_head,
            pltpu.VMEM((seqs, width), F32),
            pltpu.VMEM((seqs, width), BF16),
            dma((13,)),
            dma((chunks,)),
            dma((chunks,)),
        ],
        compiler_params=pltpu.CompilerParams(vmem_limit_bytes=VMEM_LIMIT),
        name="attention",
    )(*operands, state)


def position(sizes):
    ep = lax.axis_index("ep")
    strides = (sizes[1] * sizes[2], sizes[2], 1)
    return ep, tuple(ep // s % n for s, n in zip(strides, sizes)), strides


def greet_all(count):
    ep, tp = lax.axis_index("ep"), lax.axis_index("tp")
    barrier = pltpu.get_barrier_semaphore()

    def greet(k, carry):
        pl.semaphore_signal(
            barrier, inc=1, device_id=((ep + k) % count, tp), device_id_type=MESH
        )
        return carry

    lax.fori_loop(1, count, greet, 0)
    pl.semaphore_signal(barrier, inc=1, device_id=(ep, 1 - tp), device_id_type=MESH)
    pl.semaphore_wait(barrier, count)


def remote(src, dst, send, recv, device):
    return pltpu.make_async_remote_copy(
        src_ref=src,
        dst_ref=dst,
        send_sem=send,
        recv_sem=recv,
        device_id=device,
        device_id_type=MESH,
    )


def layer_kernel(
    sizes,
    top,
    cap,
    partial,
    hidden,
    gain,
    blend_vector,
    routing,
    route_scale,
    gate_h,
    up_h,
    down_h,
    expert_gate_h,
    expert_up_h,
    expert_down_h,
    out,
    tokens,
    own_tokens,
    metas,
    meta,
    first,
    sibling_part,
    gate_v,
    up_v,
    down_v,
    expert_gate,
    expert_up,
    expert_down,
    gate_w,
    up_w,
    mix_w,
    mix_rows,
    picked,
    from_sibling,
    lands,
    sems,
):
    (
        weight_sem,
        part_sem,
        meta_sem,
        ag_send,
        ag_recv,
        pass_send,
        pass_recv,
        pair_send,
        pair_recv,
        rs_send,
        rs_recv,
        last_sem,
    ) = sems
    chunks, across, along = sizes
    count = chunks * across * along
    plane = across * along
    ep, at, strides = position(sizes)
    tp = lax.axis_index("tp")
    half, width = first.shape
    seqs = 2 * half
    sibling = (ep, 1 - tp)
    mine = pl.ds(pl.multiple_of(tp * half, half), half)
    other = pl.ds(pl.multiple_of((1 - tp) * half, half), half)
    slots = plane * cap
    depth = gate_w.shape[0]
    units = gate_v.shape[0]
    rows_at_once = max(1, 256 // (along * seqs))
    blocks = across // rows_at_once
    block_chips = rows_at_once * along
    block_rows = block_chips * seqs
    steps = max(sizes[1:]) - 1

    weights = (
        (gate_h, gate_v),
        (up_h, up_v),
        (down_h, down_v),
        (expert_gate_h, expert_gate),
        (expert_up_h, expert_up),
        (expert_down_h, expert_down),
    )

    def weight_copy(i):
        return pltpu.make_async_copy(weights[i][0], weights[i][1], weight_sem.at[i])

    def per_core(run):
        @pl.when(tp == 0)
        def _():
            run(0)

        @pl.when(tp == 1)
        def _():
            run(1)

    order_of_planes = [0] + sorted(range(1, chunks), key=lambda k: (-min(k, chunks - k), k))

    def buffer_of(k):
        return order_of_planes.index(k) % 2

    def one_slot(k, j):
        return chunks + k * steps + j - 1

    def two_slot(k, j, i):
        return chunks * (1 + steps) + (k * steps + j - 1) * (steps + 1) + i

    def meta_copy(k):
        peer = (ep + k) % count
        return remote(meta, metas.at[ep], meta_sem.at[0], meta_sem.at[1], (peer, tp))

    gather_orders = ((0, 2, 1), (0, 1, 2))
    scatter_orders = ((1, 2), (2, 1))

    def plane_of(k):
        return (at[0] + chunks - k) % chunks

    def gather_view(core, k, i, j):
        _, d2, d3 = gather_orders[core]
        spot = [pl.ds(plane_of(k), 1), None, None]

        def one(d, back):
            return pl.ds((at[d] + sizes[d] - back) % sizes[d], 1)

        spot[d2] = pl.ds(0, sizes[d2]) if i is None else one(d2, i)
        spot[d3] = one(d3, j)
        return tokens.at[tuple(spot) + (pl.ds(core * half, half),)]

    def peer_of(d, j):
        return ep + ((at[d] + j) % sizes[d] - at[d]) * strides[d]

    def gather_copy(core, stage, k, j, i=0):
        target = gather_view(core, 0 if stage == 0 else k, i, 0)
        source = own_tokens if stage == 0 else target
        slot = (k, one_slot(k, j), two_slot(k, j, i))[stage]
        peer = peer_of(gather_orders[core][stage], j)
        return remote(source, target, ag_send.at[slot], ag_recv.at[slot], (peer, core))

    def pass_on(core, k, i, j):
        view = gather_view(core, k, i, j)
        remote(view, view, pass_send.at[k], pass_recv.at[k], sibling).start()

    def plane_pass(core, k):
        view = tokens.at[plane_of(k), :, :, pl.ds(core * half, half)]
        return remote(view, view, pass_send.at[k], pass_recv.at[k], sibling)

    def send_first(core, k):
        order = gather_orders[core]
        if k:
            gather_copy(core, 0, k, k).wait()
        for j in range(1, sizes[order[1]]):
            gather_copy(core, 1, k, j).start()
        for j in range(1, sizes[order[2]]):
            gather_copy(core, 2, k, j, 0).start()
        pass_on(core, k, 0, 0)

    def send_second(core, k):
        order = gather_orders[core]
        for i in range(1, sizes[order[1]]):
            gather_copy(core, 1, k, i).wait()
            for j in range(1, sizes[order[2]]):
                gather_copy(core, 2, k, j, i).start()
            pass_on(core, k, i, 0)

    def plane_done(core, k):
        order = gather_orders[core]
        for j in range(1, sizes[order[2]]):
            for i in range(sizes[order[1]]):
                gather_copy(core, 2, k, j, i).wait()
            pass_on(core, k, None, j)

    def plane_here(core, k):
        plane_pass(core, k).wait_send()
        plane_pass(1 - core, k).wait_recv()

    def select_of(k):
        here = metas[pl.ds(plane_of(k) * plane, plane)]
        lanes = lax.broadcasted_iota(jnp.int32, (plane, 128), 1)
        expert = ep.astype(F32)
        chosen = jnp.zeros((plane, 128), F32)
        scale_of = jnp.zeros((plane, 128), F32)
        for c in range(top):
            hit = jnp.where((here[:, c, :] == expert) & (lanes < seqs), 1.0, 0.0)
            chosen = chosen + hit
            scale_of = scale_of + hit * here[:, top + c, :]
        earlier = lax.broadcasted_iota(jnp.int32, (128, 128), 0) < lax.broadcasted_iota(
            jnp.int32, (128, 128), 1
        )
        rank = matmul(chosen.astype(BF16), jnp.where(earlier, 1.0, 0.0).astype(BF16))
        chip = lax.broadcasted_iota(jnp.int32, (plane, 128), 0).astype(F32)
        return jnp.where(chosen > 0.5, rank + chip * cap, -1.0), scale_of

    def use_tokens(k):
        z = plane_of(k)
        place, scale_of = select_of(k)
        scales = jnp.zeros((slots, 1), F32)
        for i in range(blocks):
            chips = range(i * block_chips, (i + 1) * block_chips)
            place_row = jnp.concatenate([place[p : p + 1, :seqs] for p in chips], axis=1)
            scale_row = jnp.concatenate([scale_of[p : p + 1, :seqs] for p in chips], axis=1)
            slot_of = lax.broadcasted_iota(jnp.int32, (depth, block_rows), 0).astype(F32)
            select = jnp.where(slot_of == place_row, 1.0, 0.0)
            scales = scales + jnp.sum(select[:slots] * scale_row, axis=1, keepdims=True)
            own_slots = slice(i * block_chips * cap, (i + 1) * block_chips * cap)
            own_rows = slice(i * block_rows, (i + 1) * block_rows)
            rows = tokens[z, pl.ds(i * rows_at_once, rows_at_once)].reshape(block_rows, width)
            picked[buffer_of(k), own_slots, :] = matmul(select[own_slots].astype(BF16), rows).astype(BF16)
            mix_rows[buffer_of(k), own_rows, :] = jnp.transpose(select).astype(BF16)

        def dense(i, carry):
            rows = tokens[z, pl.ds(i * rows_at_once, rows_at_once)].reshape(block_rows, width)
            gate = matmul_nt(rows, gate_w[...])
            blend = 1.0 / (1.0 + jnp.exp(-gate[:, 0:1]))
            act = silu_of(gate) * matmul_nt(rows, up_w[...]) * blend
            own_rows = pl.ds(pl.multiple_of(i * block_rows, block_rows), block_rows)
            routed = mix_rows[buffer_of(k), own_rows, :].astype(F32)
            mix_rows[buffer_of(k), own_rows, :] = (routed + act).astype(BF16)
            return carry

        lax.fori_loop(0, blocks, dense, 0)
        return scales

    def run_experts(ks, scales):
        if len(ks) == 2:
            rows = picked[...].reshape(2 * slots, width)
            scales = jnp.concatenate(scales if buffer_of(ks[0]) == 0 else scales[::-1], axis=0)
        else:
            rows, scales = picked[buffer_of(ks[0])], scales[0]
        gate = matmul(rows, expert_gate[0])
        hidden_rows = (silu_of(gate) * matmul(rows, expert_up[0])).astype(BF16)
        result = (matmul(hidden_rows, expert_down[0]) * scales).astype(BF16)
        if len(ks) == 2:
            mix_w[:, 0:slots, :] = result.reshape(2, slots, width)
        else:
            mix_w[buffer_of(ks[0]), 0:slots, :] = result

    def pair_copy(k):
        return remote(
            tokens.at[plane_of(k), :, :, other],
            from_sibling.at[k],
            pair_send.at[k],
            pair_recv.at[k],
            sibling,
        )

    def make_part(k):
        z = plane_of(k)

        def some(i, carry):
            own_rows = pl.ds(pl.multiple_of(i * block_rows, block_rows), block_rows)
            part = matmul(mix_rows[buffer_of(k), own_rows, :], mix_w[buffer_of(k)]).astype(BF16)
            ys = pl.ds(i * rows_at_once, rows_at_once)
            tokens[z, ys] = part.reshape(rows_at_once, along, seqs, width)
            return carry

        lax.fori_loop(0, blocks, some, 0)
        pair_copy(k).start()

    def spot(core, k, j=0, i=0):
        d1, d2 = scatter_orders[core]
        place = [plane_of(k), None, None]
        place[d1], place[d2] = (at[d1] + j) % sizes[d1], (at[d2] + i) % sizes[d2]
        return tuple(place) + (pl.ds(core * half, half),)

    def scatter_copy(core, stage, k, j=0, i=0):
        d1, d2 = scatter_orders[core]
        if stage == 0:
            peer, slot, target = peer_of(0, chunks - k), k, lands[2].at[k - 1]
        elif stage == 1:
            peer, slot, target = peer_of(d1, j), two_slot(k, j, i), lands[0].at[k, j - 1, i]
        else:
            peer, slot, target = peer_of(d2, i), one_slot(k, i), lands[1].at[k, i - 1]
        source = tokens.at[spot(core, k, j, i)]
        return remote(source, target, rs_send.at[slot], rs_recv.at[slot], (peer, core))

    def pair_sum(k):
        pair_copy(k).wait()
        z = plane_of(k)

        def add(b, carry):
            y, x = b // along, b % along
            tokens[z, y, x, mine, :] = (
                tokens[z, y, x, mine, :].astype(F32) + from_sibling[k, y, x].astype(F32)
            ).astype(BF16)
            return carry

        lax.fori_loop(0, plane, add, 0)

        def send(core):
            d1, d2 = scatter_orders[core]
            for i in range(sizes[d2] - 1, 0, -1):
                for j in range(1, sizes[d1]):
                    scatter_copy(core, 1, k, j, i).start()

        per_core(send)

    def send_kept(core, k):
        for j in range(1, sizes[scatter_orders[core][0]]):
            scatter_copy(core, 1, k, j, 0).start()

    def first_sum(core, k):
        d1, d2 = scatter_orders[core]
        for i in range(sizes[d2] - 1, 0, -1):
            place = spot(core, k, 0, i)
            value = tokens[place].astype(F32)
            for j in range(1, sizes[d1]):
                scatter_copy(core, 1, k, j, i).wait()
                value = value + lands[0][k, j - 1, i].astype(F32)
            tokens[place] = value.astype(BF16)
            scatter_copy(core, 2, k, 0, i).start()

    def second_sum(core, k):
        d1, d2 = scatter_orders[core]
        place = spot(core, k)
        value = tokens[place].astype(F32)
        for j in range(1, sizes[d1]):
            scatter_copy(core, 1, k, j, 0).wait()
            value = value + lands[0][k, j - 1, 0].astype(F32)
        for i in range(1, sizes[d2]):
            scatter_copy(core, 2, k, 0, i).wait()
            value = value + lands[1][k, i - 1].astype(F32)
        tokens[place] = value.astype(BF16)
        if k:
            scatter_copy(core, 0, k).start()

    def finish(core):
        value = tokens[spot(core, 0)].astype(F32) + first[...].astype(F32)
        for k in range(1, chunks):
            scatter_copy(core, 0, k).wait()
            value = value + lands[2][k - 1].astype(F32)
        out[pl.ds(core * half, half), :] = value.astype(BF16)

    for i in range(6):
        weight_copy(i).start()
    meta[...] = jnp.zeros(meta.shape, F32)
    meta[0:top, 0:seqs] = routing[...].astype(F32)
    meta[top : 2 * top, 0:seqs] = route_scale[...]
    base = hidden[mine, :].astype(F32) + partial[mine, :].astype(F32)
    greet_all(count)
    swap = remote(partial.at[other], sibling_part, part_sem.at[0], part_sem.at[1], sibling)
    swap.start()

    def start_meta(k, carry):
        meta_copy(k).start()
        return carry

    lax.fori_loop(1, count, start_meta, 0)
    swap.wait()
    total = (base + sibling_part[...].astype(F32)).astype(BF16)
    first[...] = total
    normed = rms_scaled(total.astype(F32), gain[...]).astype(BF16)
    own_tokens[0, 0, 0] = normed
    tokens[at[0], at[1], at[2], mine, :] = normed

    def start_planes(core):
        send_first(core, 0)
        for k in order_of_planes[1:]:
            gather_copy(core, 0, k, k).start()

    per_core(start_planes)
    metas[ep] = meta[...]
    for i in range(3):
        weight_copy(i).wait()
    blend_row = jnp.concatenate(
        [blend_vector[i : i + 1, :].astype(F32) for i in range(width // 128)], axis=1
    )
    top_row = lax.broadcasted_iota(jnp.int32, (slots, width), 0) == 0
    gate_w[0:slots, :] = jnp.where(top_row, blend_row, 0.0).astype(BF16)
    up_w[0:slots, :] = jnp.zeros((slots, width), BF16)
    if slots + units < depth:
        rest = (depth - slots - units, width)
        gate_w[slots + units : depth, :] = jnp.zeros(rest, BF16)
        up_w[slots + units : depth, :] = jnp.zeros(rest, BF16)
        for b in range(2):
            mix_w[b, slots + units : depth, :] = jnp.zeros(rest, BF16)
    gate_w[slots : slots + units, :] = gate_v[...]
    up_w[slots : slots + units, :] = up_v[...]
    for b in range(2):
        mix_w[b, slots : slots + units, :] = down_v[...]

    def on_core(run, k):
        if 0 <= k < chunks:
            per_core(functools.partial(run, k=order_of_planes[k]))

    def pair_step(k):
        if 0 <= k < chunks:
            pair_sum(order_of_planes[k])
            on_core(send_kept, k)

    joint = [k for k in (chunks - 2, chunks - 1) if k > 0]
    on_core(send_second, 0)
    on_core(send_first, 1)
    on_core(send_second, 1)
    on_core(plane_done, 0)
    on_core(send_first, 2)
    some = metas.at[pl.ds(0, count - 1)]
    remote(some, some, meta_sem.at[0], meta_sem.at[1], sibling).wait()
    for i in range(3, 6):
        weight_copy(i).wait()
    on_core(plane_here, 0)
    scales = [use_tokens(0)]
    on_core(send_second, 2)
    on_core(send_first, 3)
    on_core(plane_done, 1)
    run_experts([0], scales)
    make_part(0)
    for k in range(1, chunks - 2):
        on_core(plane_here, k)
        scales = [use_tokens(order_of_planes[k])]
        on_core(send_second, k + 2)
        on_core(send_first, k + 3)
        pair_step(k - 1)
        on_core(first_sum, k - 2)
        run_experts([order_of_planes[k]], scales)
        on_core(plane_done, k + 1)
        make_part(order_of_planes[k])
    scales = []
    for k in joint:
        on_core(plane_here, k)
        scales.append(use_tokens(order_of_planes[k]))
        if k == joint[0]:
            pair_step(k - 1)
            on_core(plane_done, k + 1)
            on_core(first_sum, k - 2)
    if joint:
        run_experts([order_of_planes[k] for k in joint], scales)
    for k in joint:
        make_part(order_of_planes[k])
    on_core(first_sum, chunks - 3)
    for k in joint or [0]:
        pair_sum(order_of_planes[k])
    for k in joint or [0]:
        on_core(send_kept, k)
    on_core(second_sum, chunks - 4)
    on_core(second_sum, chunks - 3)
    for k in joint or [0]:
        on_core(first_sum, k)
    for k in joint or [0]:
        on_core(second_sum, k)
    per_core(finish)

    last = remote(out.at[mine], out.at[mine], last_sem.at[0], last_sem.at[1], sibling)
    last.start()
    last.wait()


def layer_after(sizes, partial, hidden, gain, blend_vector, routing, route_scale, weights):
    seqs, width = hidden.shape
    count = sizes[0] * sizes[1] * sizes[2]
    half, top = seqs // 2, routing.shape[0]
    cap = max(2, 2 * seqs * top // count)
    plane = sizes[1] * sizes[2]
    slots = plane * cap
    depth = -(-(slots + weights[0].shape[0]) // 128) * 128
    chunks, side, block = sizes[0], max(sizes[1:]), (half, width)
    dma = pltpu.SemaphoreType.DMA
    any_spec = pl.BlockSpec(memory_space=pl.ANY)
    hop = dma((chunks * (side * side),))
    return pl.pallas_call(
        functools.partial(layer_kernel, sizes, top, cap),
        out_shape=jax.ShapeDtypeStruct((seqs, width), BF16),
        in_specs=[VMEM_SPEC] * 6 + [any_spec] * 6,
        out_specs=VMEM_SPEC,
        scratch_shapes=[
            pltpu.VMEM(sizes + (seqs, width), BF16),
            pltpu.VMEM((1, 1, 1) + block, BF16),
            pltpu.VMEM((count, 8, 128), F32),
            pltpu.VMEM((8, 128), F32),
            pltpu.VMEM(block, BF16),
            pltpu.VMEM(block, BF16),
        ]
        + [pltpu.VMEM(w.shape, BF16) for w in weights]
        + [
            pltpu.VMEM((depth, width), BF16),
            pltpu.VMEM((depth, width), BF16),
            pltpu.VMEM((2, depth, width), BF16),
            pltpu.VMEM((2, plane * seqs, depth), BF16),
            pltpu.VMEM((2, slots, width), BF16),
            pltpu.VMEM(sizes + block, BF16),
            [
                pltpu.VMEM((chunks, max(1, side - 1), side) + block, BF16),
                pltpu.VMEM((chunks, max(1, side - 1)) + block, BF16),
                pltpu.VMEM((max(1, chunks - 1),) + block, BF16),
            ],
            [
                dma((6,)),
                dma((2,)),
                dma((2,)),
                hop,
                hop,
                dma((chunks,)),
                dma((chunks,)),
                dma((chunks,)),
                dma((chunks,)),
                hop,
                hop,
                dma((2,)),
            ],
        ],
        compiler_params=pltpu.CompilerParams(
            collective_id=0, has_side_effects=True, vmem_limit_bytes=VMEM_LIMIT
        ),
        name="layer_after",
    )(partial, hidden, gain, blend_vector, routing, route_scale, *weights)


def shards(
    hidden,
    mix_gain,
    recept_weight,
    key_weight,
    value_weight,
    decay_down,
    decay_up,
    decay_bias,
    rate_down,
    rate_up,
    rate_bias,
    head_gain,
    out_weight,
    memory_state,
    ffn_gain,
    blend_vector,
    dense_gate,
    dense_up,
    dense_down,
    expert_gate,
    expert_up,
    expert_down,
    routing,
    route_scale,
):
    sizes = factors_of(lax.axis_size("ep"))
    new_state, partial = attention(
        (
            hidden,
            mix_gain[None],
            decay_down.T,
            rate_down.T,
            decay_up,
            rate_up,
            decay_bias[None],
            rate_bias[None],
            recept_weight,
            key_weight,
            value_weight,
            head_gain[None],
            out_weight,
        ),
        memory_state,
    )
    layer_out = layer_after(
        sizes,
        partial,
        hidden,
        ffn_gain[None],
        blend_vector.reshape(-1, 128),
        routing.T,
        route_scale.T,
        (dense_gate.T, dense_up.T, dense_down, expert_gate, expert_up, expert_down),
    )
    return (layer_out, new_state)


def solution(mesh):
    in_specs = (
        P("ep", None),
        P(),
        P(None, "tp"),
        P(None, "tp"),
        P(None, "tp"),
        P(),
        P(),
        P(),
        P(),
        P(),
        P(),
        P(),
        P("tp", None),
        P("ep", "tp", None, None),
        P(),
        P(),
        P(None, ("ep", "tp")),
        P(None, ("ep", "tp")),
        P(("ep", "tp"), None),
        P("ep", None, "tp"),
        P("ep", None, "tp"),
        P("ep", "tp", None),
        P("ep", None),
        P("ep", None),
    )
    out_specs = (P("ep", None), P("ep", "tp", None, None))
    return jax.shard_map(shards, mesh=mesh, in_specs=in_specs, out_specs=out_specs, check_vma=False)
```

```python
import functools
import math

import jax
import jax.numpy as jnp
from jax import lax
from jax.experimental import pallas as pl
from jax.experimental.pallas import tpu as pltpu
from jax.sharding import PartitionSpec as P

MESH = pl.DeviceIdType.MESH
F32 = jnp.float32
BF16 = jnp.bfloat16
VMEM_LIMIT = 64 * 1024 * 1024 - 65536
VMEM_SPEC = pl.BlockSpec(memory_space=pltpu.VMEM)


def matmul(left, right):
    return jnp.dot(left, right, preferred_element_type=F32)


def matmul_nt(left, right):
    return lax.dot_general(left, right, (((1,), (1,)), ((), ())), preferred_element_type=F32)


def silu_of(tensor):
    return tensor / (1.0 + jnp.exp(-tensor))


def rms_scaled(values, gain):
    return values * lax.rsqrt(jnp.mean(values * values, axis=-1, keepdims=True) + 1e-06) * gain


def factors_of(count):
    slow = 4 if count % 4 == 0 else 1
    rest = count // slow
    mid = math.isqrt(rest)
    while rest % mid:
        mid -= 1
    return slow, mid, rest // mid


def attention_kernel(chunks, *refs):
    sources, (state_h, state_out_h, partial), rest = refs[:13], refs[13:16], refs[16:]
    local, rest = rest[:13], rest[13:]
    state_v, new_v, recept_s, pull_s, key_rate_s, value_s, decay_s, readout_s, normed_s = rest[:9]
    part_sem, in_sem, out_sem = rest[9:]
    (
        hidden,
        mix_gain,
        decay_down,
        rate_down,
        decay_up,
        rate_up,
        decay_bias,
        rate_bias,
        recept_weight,
        key_weight,
        value_weight,
        head_gain,
        out_weight,
    ) = local
    heads, seqs, size = pull_s.shape
    width = heads * size
    step_rows = seqs // chunks
    own = pl.ds(pl.multiple_of(lax.axis_index("tp") * width, 128), width)

    def part_copy(i):
        return pltpu.make_async_copy(sources[i], local[i], part_sem.at[i])

    def rows_of(c):
        return pl.ds(c * step_rows, step_rows)

    def in_copy(c):
        return pltpu.make_async_copy(state_h.at[rows_of(c)], state_v.at[rows_of(c)], in_sem.at[c])

    def out_copy(c):
        return pltpu.make_async_copy(new_v.at[rows_of(c)], state_out_h.at[rows_of(c)], out_sem.at[c])

    for i in range(11):
        part_copy(i).start()

    def start_in(c, carry):
        in_copy(c).start()
        return carry

    lax.fori_loop(0, chunks, start_in, 0)
    part_copy(11).start()
    part_copy(12).start()

    part_copy(0).wait()
    part_copy(1).wait()
    normed = rms_scaled(hidden[...].astype(F32), mix_gain[...]).astype(BF16)
    for i in range(2, 8):
        part_copy(i).wait()
    decay_low = jnp.tanh(matmul_nt(normed, decay_down[...])).astype(BF16)
    decay_pre = matmul(decay_low, decay_up[:, own]) + decay_bias[:, own]
    decay = jnp.exp(-math.exp(-0.5) / (1.0 + jnp.exp(-decay_pre)))
    rate_low = matmul_nt(normed, rate_down[...]).astype(BF16)
    rate = 1.0 / (1.0 + jnp.exp(-(matmul(rate_low, rate_up[:, own]) + rate_bias[:, own])))
    part_copy(8).wait()
    recept = matmul(normed, recept_weight[...]).astype(BF16).astype(F32)
    part_copy(9).wait()
    keys = matmul(normed, key_weight[...]).astype(BF16).astype(F32)
    part_copy(10).wait()
    vals = matmul(normed, value_weight[...]).astype(BF16).astype(F32)
    for h in range(heads):
        cols = slice(h * size, (h + 1) * size)
        key_h = keys[:, cols]
        inverse = 1.0 / (jnp.sum(key_h * key_h, axis=-1, keepdims=True) + 1e-06)
        recept_s[:, h, :] = recept[:, cols]
        pull_s[h] = key_h * inverse
        key_rate_s[h] = key_h * rate[:, cols]
        value_s[h] = vals[:, cols]
        decay_s[h] = decay[:, cols]

    shape, flat = (heads, size, size), (heads * size, size)
    eye = lax.broadcasted_iota(jnp.int32, shape, 1) == lax.broadcasted_iota(jnp.int32, shape, 2)
    spread = (heads, width)
    owner = lax.broadcasted_iota(jnp.int32, spread, 0)
    own_lanes = owner == lax.broadcasted_iota(jnp.int32, spread, 1) // size

    def one_sequence(row):
        here = pl.ds(row, 1)
        state = state_v[row]
        gain = jnp.sum(
            jnp.where(eye, value_s[:, here], 0.0) - state * pull_s[:, here], axis=-1, keepdims=True
        )
        new = state * decay_s[:, here] + gain * key_rate_s[:, here]
        new_v[row] = new
        out = matmul_nt(recept_s[row].astype(BF16), new.astype(BF16).reshape(flat))
        readout_s[here, :] = jnp.sum(jnp.where(own_lanes, out, 0.0), axis=0, keepdims=True)

    def one_chunk(c, carry):
        in_copy(c).wait()

        def some(k, inner):
            for j in range(4):
                one_sequence(c * step_rows + k * 4 + j)
            return inner

        lax.fori_loop(0, step_rows // 4, some, 0)
        out_copy(c).start()
        return carry

    lax.fori_loop(0, chunks, one_chunk, 0)

    part_copy(11).wait()
    gain = head_gain[:, own]
    for h in range(heads):
        cols = slice(h * size, (h + 1) * size)
        out = readout_s[:, cols]
        centred = out - jnp.mean(out, axis=-1, keepdims=True)
        variance = jnp.mean(centred * centred, axis=-1, keepdims=True)
        normed_s[:, cols] = (centred * lax.rsqrt(variance + 0.00064) * gain[:, cols]).astype(BF16)
    part_copy(12).wait()
    partial[...] = matmul(normed_s[...], out_weight[...]).astype(BF16)

    def wait_out(c, carry):
        out_copy(c).wait()
        return carry

    lax.fori_loop(0, chunks, wait_out, 0)


def attention(operands, state):
    seqs, heads, size, _ = state.shape
    hidden = operands[0]
    width = heads * size
    chunks = seqs // math.gcd(seqs, 4)
    per_head = pltpu.VMEM((heads, seqs, size), F32)
    dma = pltpu.SemaphoreType.DMA
    any_spec = pl.BlockSpec(memory_space=pl.ANY)
    return pl.pallas_call(
        functools.partial(attention_kernel, chunks),
        out_shape=(
            jax.ShapeDtypeStruct(state.shape, F32),
            jax.ShapeDtypeStruct(hidden.shape, BF16),
        ),
        in_specs=[any_spec] * 14,
        out_specs=(any_spec, VMEM_SPEC),
        scratch_shapes=[pltpu.VMEM(a.shape, a.dtype) for a in operands]
        + [
            pltpu.VMEM(state.shape, F32),
            pltpu.VMEM(state.shape, F32),
            pltpu.VMEM((seqs, heads, size), F32),
            per_head,
            per_head,
            per_head,
            per_head,
            pltpu.VMEM((seqs, width), F32),
            pltpu.VMEM((seqs, width), BF16),
            dma((13,)),
            dma((chunks,)),
            dma((chunks,)),
        ],
        compiler_params=pltpu.CompilerParams(vmem_limit_bytes=VMEM_LIMIT),
        name="attention",
    )(*operands, state)


def position(sizes):
    ep = lax.axis_index("ep")
    strides = (sizes[1] * sizes[2], sizes[2], 1)
    return ep, tuple(ep // s % n for s, n in zip(strides, sizes)), strides


def greet_all(count):
    ep, tp = lax.axis_index("ep"), lax.axis_index("tp")
    barrier = pltpu.get_barrier_semaphore()

    def greet(k, carry):
        pl.semaphore_signal(
            barrier, inc=1, device_id=((ep + k) % count, tp), device_id_type=MESH
        )
        return carry

    lax.fori_loop(1, count, greet, 0)
    pl.semaphore_signal(barrier, inc=1, device_id=(ep, 1 - tp), device_id_type=MESH)
    pl.semaphore_wait(barrier, count)


def remote(src, dst, send, recv, device):
    return pltpu.make_async_remote_copy(
        src_ref=src,
        dst_ref=dst,
        send_sem=send,
        recv_sem=recv,
        device_id=device,
        device_id_type=MESH,
    )


def layer_kernel(
    sizes,
    top,
    cap,
    partial,
    hidden,
    gain,
    blend_vector,
    routing,
    route_scale,
    gate_h,
    up_h,
    down_h,
    expert_gate_h,
    expert_up_h,
    expert_down_h,
    out,
    tokens,
    own_tokens,
    metas,
    meta,
    first,
    sibling_part,
    gate_v,
    up_v,
    down_v,
    expert_gate,
    expert_up,
    expert_down,
    gate_w,
    up_w,
    mix_w,
    mix_rows,
    picked,
    from_sibling,
    lands,
    sems,
):
    (
        weight_sem,
        part_sem,
        meta_sem,
        ag_send,
        ag_recv,
        pass_send,
        pass_recv,
        pair_send,
        pair_recv,
        rs_send,
        rs_recv,
        last_sem,
    ) = sems
    chunks, across, along = sizes
    count = chunks * across * along
    plane = across * along
    ep, at, strides = position(sizes)
    tp = lax.axis_index("tp")
    half, width = first.shape
    seqs = 2 * half
    sibling = (ep, 1 - tp)
    mine = pl.ds(pl.multiple_of(tp * half, half), half)
    other = pl.ds(pl.multiple_of((1 - tp) * half, half), half)
    slots = plane * cap
    depth = gate_w.shape[0]
    units = gate_v.shape[0]
    rows_at_once = max(1, 256 // (along * seqs))
    blocks = across // rows_at_once
    block_chips = rows_at_once * along
    block_rows = block_chips * seqs
    steps = max(sizes[1:]) - 1

    weights = (
        (gate_h, gate_v),
        (up_h, up_v),
        (down_h, down_v),
        (expert_gate_h, expert_gate),
        (expert_up_h, expert_up),
        (expert_down_h, expert_down),
    )

    def weight_copy(i):
        return pltpu.make_async_copy(weights[i][0], weights[i][1], weight_sem.at[i])

    def per_core(run):
        @pl.when(tp == 0)
        def _():
            run(0)

        @pl.when(tp == 1)
        def _():
            run(1)

    order_of_planes = [0] + sorted(range(1, chunks), key=lambda k: (-min(k, chunks - k), k))

    def buffer_of(k):
        return order_of_planes.index(k) % 2

    def one_slot(k, j):
        return chunks + k * steps + j - 1

    def two_slot(k, j, i):
        return chunks * (1 + steps) + (k * steps + j - 1) * (steps + 1) + i

    def meta_copy(k):
        peer = (ep + k) % count
        return remote(meta, metas.at[ep], meta_sem.at[0], meta_sem.at[1], (peer, tp))

    gather_orders = ((0, 2, 1), (0, 1, 2))
    scatter_orders = ((1, 2), (2, 1))

    def plane_of(k):
        return (at[0] + chunks - k) % chunks

    def gather_view(core, k, i, j):
        _, d2, d3 = gather_orders[core]
        spot = [pl.ds(plane_of(k), 1), None, None]

        def one(d, back):
            return pl.ds((at[d] + sizes[d] - back) % sizes[d], 1)

        spot[d2] = pl.ds(0, sizes[d2]) if i is None else one(d2, i)
        spot[d3] = one(d3, j)
        return tokens.at[tuple(spot) + (pl.ds(core * half, half),)]

    def peer_of(d, j):
        return ep + ((at[d] + j) % sizes[d] - at[d]) * strides[d]

    def gather_copy(core, stage, k, j, i=0):
        target = gather_view(core, 0 if stage == 0 else k, i, 0)
        source = own_tokens if stage == 0 else target
        slot = (k, one_slot(k, j), two_slot(k, j, i))[stage]
        peer = peer_of(gather_orders[core][stage], j)
        return remote(source, target, ag_send.at[slot], ag_recv.at[slot], (peer, core))

    def pass_on(core, k, i, j):
        view = gather_view(core, k, i, j)
        remote(view, view, pass_send.at[k], pass_recv.at[k], sibling).start()

    def plane_pass(core, k):
        view = tokens.at[plane_of(k), :, :, pl.ds(core * half, half)]
        return remote(view, view, pass_send.at[k], pass_recv.at[k], sibling)

    def send_first(core, k):
        order = gather_orders[core]
        if k:
            gather_copy(core, 0, k, k).wait()
        for j in range(1, sizes[order[1]]):
            gather_copy(core, 1, k, j).start()
        for j in range(1, sizes[order[2]]):
            gather_copy(core, 2, k, j, 0).start()
        pass_on(core, k, 0, 0)

    def send_second(core, k):
        order = gather_orders[core]
        for i in range(1, sizes[order[1]]):
            gather_copy(core, 1, k, i).wait()
            for j in range(1, sizes[order[2]]):
                gather_copy(core, 2, k, j, i).start()
            pass_on(core, k, i, 0)

    def plane_done(core, k):
        order = gather_orders[core]
        for j in range(1, sizes[order[2]]):
            for i in range(sizes[order[1]]):
                gather_copy(core, 2, k, j, i).wait()
            pass_on(core, k, None, j)

    def plane_here(core, k):
        plane_pass(core, k).wait_send()
        plane_pass(1 - core, k).wait_recv()

    def select_of(k):
        here = metas[pl.ds(plane_of(k) * plane, plane)]
        lanes = lax.broadcasted_iota(jnp.int32, (plane, 128), 1)
        expert = ep.astype(F32)
        chosen = jnp.zeros((plane, 128), F32)
        scale_of = jnp.zeros((plane, 128), F32)
        for c in range(top):
            hit = jnp.where((here[:, c, :] == expert) & (lanes < seqs), 1.0, 0.0)
            chosen = chosen + hit
            scale_of = scale_of + hit * here[:, top + c, :]
        earlier = lax.broadcasted_iota(jnp.int32, (128, 128), 0) < lax.broadcasted_iota(
            jnp.int32, (128, 128), 1
        )
        rank = matmul(chosen.astype(BF16), jnp.where(earlier, 1.0, 0.0).astype(BF16))
        chip = lax.broadcasted_iota(jnp.int32, (plane, 128), 0).astype(F32)
        return jnp.where(chosen > 0.5, rank + chip * cap, -1.0), scale_of

    def use_tokens(k):
        z = plane_of(k)
        place, scale_of = select_of(k)
        scales = jnp.zeros((slots, 1), F32)
        for i in range(blocks):
            chips = range(i * block_chips, (i + 1) * block_chips)
            place_row = jnp.concatenate([place[p : p + 1, :seqs] for p in chips], axis=1)
            scale_row = jnp.concatenate([scale_of[p : p + 1, :seqs] for p in chips], axis=1)
            slot_of = lax.broadcasted_iota(jnp.int32, (depth, block_rows), 0).astype(F32)
            select = jnp.where(slot_of == place_row, 1.0, 0.0)
            scales = scales + jnp.sum(select[:slots] * scale_row, axis=1, keepdims=True)
            own_slots = slice(i * block_chips * cap, (i + 1) * block_chips * cap)
            own_rows = slice(i * block_rows, (i + 1) * block_rows)
            rows = tokens[z, pl.ds(i * rows_at_once, rows_at_once)].reshape(block_rows, width)
            picked[buffer_of(k), own_slots, :] = matmul(select[own_slots].astype(BF16), rows).astype(BF16)
            mix_rows[buffer_of(k), own_rows, :] = jnp.transpose(select).astype(BF16)

        def dense(i, carry):
            rows = tokens[z, pl.ds(i * rows_at_once, rows_at_once)].reshape(block_rows, width)
            gate = matmul_nt(rows, gate_w[...])
            blend = 1.0 / (1.0 + jnp.exp(-gate[:, 0:1]))
            act = silu_of(gate) * matmul_nt(rows, up_w[...]) * blend
            own_rows = pl.ds(pl.multiple_of(i * block_rows, block_rows), block_rows)
            routed = mix_rows[buffer_of(k), own_rows, :].astype(F32)
            mix_rows[buffer_of(k), own_rows, :] = (routed + act).astype(BF16)
            return carry

        lax.fori_loop(0, blocks, dense, 0)
        return scales

    def run_experts(ks, scales):
        if len(ks) == 2:
            rows = picked[...].reshape(2 * slots, width)
            scales = jnp.concatenate(scales if buffer_of(ks[0]) == 0 else scales[::-1], axis=0)
        else:
            rows, scales = picked[buffer_of(ks[0])], scales[0]
        gate = matmul(rows, expert_gate[0])
        hidden_rows = (silu_of(gate) * matmul(rows, expert_up[0])).astype(BF16)
        result = (matmul(hidden_rows, expert_down[0]) * scales).astype(BF16)
        if len(ks) == 2:
            mix_w[:, 0:slots, :] = result.reshape(2, slots, width)
        else:
            mix_w[buffer_of(ks[0]), 0:slots, :] = result

    def pair_copy(k):
        return remote(
            tokens.at[plane_of(k), :, :, other],
            from_sibling.at[k],
            pair_send.at[k],
            pair_recv.at[k],
            sibling,
        )

    def make_part(k):
        z = plane_of(k)

        def some(i, carry):
            own_rows = pl.ds(pl.multiple_of(i * block_rows, block_rows), block_rows)
            part = matmul(mix_rows[buffer_of(k), own_rows, :], mix_w[buffer_of(k)]).astype(BF16)
            ys = pl.ds(i * rows_at_once, rows_at_once)
            tokens[z, ys] = part.reshape(rows_at_once, along, seqs, width)
            return carry

        lax.fori_loop(0, blocks, some, 0)
        pair_copy(k).start()

    def spot(core, k, j=0, i=0):
        d1, d2 = scatter_orders[core]
        place = [plane_of(k), None, None]
        place[d1], place[d2] = (at[d1] + j) % sizes[d1], (at[d2] + i) % sizes[d2]
        return tuple(place) + (pl.ds(core * half, half),)

    def scatter_copy(core, stage, k, j=0, i=0):
        d1, d2 = scatter_orders[core]
        if stage == 0:
            peer, slot, target = peer_of(0, chunks - k), k, lands[2].at[k - 1]
        elif stage == 1:
            peer, slot, target = peer_of(d1, j), two_slot(k, j, i), lands[0].at[k, j - 1, i]
        else:
            peer, slot, target = peer_of(d2, i), one_slot(k, i), lands[1].at[k, i - 1]
        source = tokens.at[spot(core, k, j, i)]
        return remote(source, target, rs_send.at[slot], rs_recv.at[slot], (peer, core))

    def pair_sum(k):
        pair_copy(k).wait()
        z = plane_of(k)

        def add(b, carry):
            y, x = b // along, b % along
            tokens[z, y, x, mine, :] = (
                tokens[z, y, x, mine, :].astype(F32) + from_sibling[k, y, x].astype(F32)
            ).astype(BF16)
            return carry

        lax.fori_loop(0, plane, add, 0)

        def send(core):
            d1, d2 = scatter_orders[core]
            for i in range(sizes[d2] - 1, 0, -1):
                for j in range(1, sizes[d1]):
                    scatter_copy(core, 1, k, j, i).start()

        per_core(send)

    def send_kept(core, k):
        for j in range(1, sizes[scatter_orders[core][0]]):
            scatter_copy(core, 1, k, j, 0).start()

    def first_sum(core, k):
        d1, d2 = scatter_orders[core]
        for i in range(sizes[d2] - 1, 0, -1):
            place = spot(core, k, 0, i)
            value = tokens[place].astype(F32)
            for j in range(1, sizes[d1]):
                scatter_copy(core, 1, k, j, i).wait()
                value = value + lands[0][k, j - 1, i].astype(F32)
            tokens[place] = value.astype(BF16)
            scatter_copy(core, 2, k, 0, i).start()

    def second_sum(core, k):
        d1, d2 = scatter_orders[core]
        place = spot(core, k)
        value = tokens[place].astype(F32)
        for j in range(1, sizes[d1]):
            scatter_copy(core, 1, k, j, 0).wait()
            value = value + lands[0][k, j - 1, 0].astype(F32)
        for i in range(1, sizes[d2]):
            scatter_copy(core, 2, k, 0, i).wait()
            value = value + lands[1][k, i - 1].astype(F32)
        tokens[place] = value.astype(BF16)
        if k:
            scatter_copy(core, 0, k).start()

    def finish(core):
        value = tokens[spot(core, 0)].astype(F32) + first[...].astype(F32)
        for k in range(1, chunks):
            scatter_copy(core, 0, k).wait()
            value = value + lands[2][k - 1].astype(F32)
        out[pl.ds(core * half, half), :] = value.astype(BF16)

    for i in range(6):
        weight_copy(i).start()
    meta[...] = jnp.zeros(meta.shape, F32)
    meta[0:top, 0:seqs] = routing[...].astype(F32)
    meta[top : 2 * top, 0:seqs] = route_scale[...]
    base = hidden[mine, :].astype(F32) + partial[mine, :].astype(F32)
    greet_all(count)
    swap = remote(partial.at[other], sibling_part, part_sem.at[0], part_sem.at[1], sibling)
    swap.start()

    def start_meta(k, carry):
        meta_copy(k).start()
        return carry

    lax.fori_loop(1, count, start_meta, 0)
    swap.wait()
    total = (base + sibling_part[...].astype(F32)).astype(BF16)
    first[...] = total
    normed = rms_scaled(total.astype(F32), gain[...]).astype(BF16)
    own_tokens[0, 0, 0] = normed
    tokens[at[0], at[1], at[2], mine, :] = normed

    def start_planes(core):
        send_first(core, 0)
        for k in order_of_planes[1:]:
            gather_copy(core, 0, k, k).start()

    per_core(start_planes)
    metas[ep] = meta[...]
    for i in range(3):
        weight_copy(i).wait()
    blend_row = jnp.concatenate(
        [blend_vector[i : i + 1, :].astype(F32) for i in range(width // 128)], axis=1
    )
    top_row = lax.broadcasted_iota(jnp.int32, (slots, width), 0) == 0
    gate_w[0:slots, :] = jnp.where(top_row, blend_row, 0.0).astype(BF16)
    up_w[0:slots, :] = jnp.zeros((slots, width), BF16)
    if slots + units < depth:
        rest = (depth - slots - units, width)
        gate_w[slots + units : depth, :] = jnp.zeros(rest, BF16)
        up_w[slots + units : depth, :] = jnp.zeros(rest, BF16)
        for b in range(2):
            mix_w[b, slots + units : depth, :] = jnp.zeros(rest, BF16)
    gate_w[slots : slots + units, :] = gate_v[...]
    up_w[slots : slots + units, :] = up_v[...]
    for b in range(2):
        mix_w[b, slots : slots + units, :] = down_v[...]

    def on_core(run, k):
        if 0 <= k < chunks:
            per_core(functools.partial(run, k=order_of_planes[k]))

    def pair_step(k):
        if 0 <= k < chunks:
            pair_sum(order_of_planes[k])
            on_core(send_kept, k)

    joint = [k for k in (chunks - 2, chunks - 1) if k > 0]
    on_core(send_second, 0)
    on_core(send_first, 1)
    on_core(send_second, 1)
    on_core(plane_done, 0)
    on_core(send_first, 2)
    some = metas.at[pl.ds(0, count - 1)]
    remote(some, some, meta_sem.at[0], meta_sem.at[1], sibling).wait()
    for i in range(3, 6):
        weight_copy(i).wait()
    on_core(plane_here, 0)
    scales = [use_tokens(0)]
    on_core(send_second, 2)
    on_core(send_first, 3)
    on_core(plane_done, 1)
    run_experts([0], scales)
    make_part(0)
    for k in range(1, chunks - 2):
        on_core(plane_here, k)
        scales = [use_tokens(order_of_planes[k])]
        on_core(send_second, k + 2)
        on_core(send_first, k + 3)
        pair_step(k - 1)
        on_core(first_sum, k - 2)
        run_experts([order_of_planes[k]], scales)
        on_core(plane_done, k + 1)
        make_part(order_of_planes[k])
    scales = []
    for k in joint:
        on_core(plane_here, k)
        scales.append(use_tokens(order_of_planes[k]))
        if k == joint[0]:
            pair_step(k - 1)
            on_core(plane_done, k + 1)
            on_core(first_sum, k - 2)
    if joint:
        run_experts([order_of_planes[k] for k in joint], scales)
    for k in joint:
        make_part(order_of_planes[k])
    on_core(first_sum, chunks - 3)
    for k in joint or [0]:
        pair_step(k)
    on_core(second_sum, chunks - 4)
    on_core(second_sum, chunks - 3)
    for k in joint or [0]:
        on_core(first_sum, k)
    for k in joint or [0]:
        on_core(second_sum, k)
    per_core(finish)

    last = remote(out.at[mine], out.at[mine], last_sem.at[0], last_sem.at[1], sibling)
    last.start()
    last.wait()


def layer_after(sizes, partial, hidden, gain, blend_vector, routing, route_scale, weights):
    seqs, width = hidden.shape
    count = sizes[0] * sizes[1] * sizes[2]
    half, top = seqs // 2, routing.shape[0]
    cap = max(2, 2 * seqs * top // count)
    plane = sizes[1] * sizes[2]
    slots = plane * cap
    depth = -(-(slots + weights[0].shape[0]) // 128) * 128
    chunks, side, block = sizes[0], max(sizes[1:]), (half, width)
    dma = pltpu.SemaphoreType.DMA
    any_spec = pl.BlockSpec(memory_space=pl.ANY)
    hop = dma((chunks * (side * side),))
    return pl.pallas_call(
        functools.partial(layer_kernel, sizes, top, cap),
        out_shape=jax.ShapeDtypeStruct((seqs, width), BF16),
        in_specs=[VMEM_SPEC] * 6 + [any_spec] * 6,
        out_specs=VMEM_SPEC,
        scratch_shapes=[
            pltpu.VMEM(sizes + (seqs, width), BF16),
            pltpu.VMEM((1, 1, 1) + block, BF16),
            pltpu.VMEM((count, 8, 128), F32),
            pltpu.VMEM((8, 128), F32),
            pltpu.VMEM(block, BF16),
            pltpu.VMEM(block, BF16),
        ]
        + [pltpu.VMEM(w.shape, BF16) for w in weights]
        + [
            pltpu.VMEM((depth, width), BF16),
            pltpu.VMEM((depth, width), BF16),
            pltpu.VMEM((2, depth, width), BF16),
            pltpu.VMEM((2, plane * seqs, depth), BF16),
            pltpu.VMEM((2, slots, width), BF16),
            pltpu.VMEM(sizes + block, BF16),
            [
                pltpu.VMEM((chunks, max(1, side - 1), side) + block, BF16),
                pltpu.VMEM((chunks, max(1, side - 1)) + block, BF16),
                pltpu.VMEM((max(1, chunks - 1),) + block, BF16),
            ],
            [
                dma((6,)),
                dma((2,)),
                dma((2,)),
                hop,
                hop,
                dma((chunks,)),
                dma((chunks,)),
                dma((chunks,)),
                dma((chunks,)),
                hop,
                hop,
                dma((2,)),
            ],
        ],
        compiler_params=pltpu.CompilerParams(
            collective_id=0, has_side_effects=True, vmem_limit_bytes=VMEM_LIMIT
        ),
        name="layer_after",
    )(partial, hidden, gain, blend_vector, routing, route_scale, *weights)


def shards(
    hidden,
    mix_gain,
    recept_weight,
    key_weight,
    value_weight,
    decay_down,
    decay_up,
    decay_bias,
    rate_down,
    rate_up,
    rate_bias,
    head_gain,
    out_weight,
    memory_state,
    ffn_gain,
    blend_vector,
    dense_gate,
    dense_up,
    dense_down,
    expert_gate,
    expert_up,
    expert_down,
    routing,
    route_scale,
):
    sizes = factors_of(lax.axis_size("ep"))
    new_state, partial = attention(
        (
            hidden,
            mix_gain[None],
            decay_down.T,
            rate_down.T,
            decay_up,
            rate_up,
            decay_bias[None],
            rate_bias[None],
            recept_weight,
            key_weight,
            value_weight,
            head_gain[None],
            out_weight,
        ),
        memory_state,
    )
    layer_out = layer_after(
        sizes,
        partial,
        hidden,
        ffn_gain[None],
        blend_vector.reshape(-1, 128),
        routing.T,
        route_scale.T,
        (dense_gate.T, dense_up.T, dense_down, expert_gate, expert_up, expert_down),
    )
    return (layer_out, new_state)


def solution(mesh):
    in_specs = (
        P("ep", None),
        P(),
        P(None, "tp"),
        P(None, "tp"),
        P(None, "tp"),
        P(),
        P(),
        P(),
        P(),
        P(),
        P(),
        P(),
        P("tp", None),
        P("ep", "tp", None, None),
        P(),
        P(),
        P(None, ("ep", "tp")),
        P(None, ("ep", "tp")),
        P(("ep", "tp"), None),
        P("ep", None, "tp"),
        P("ep", None, "tp"),
        P("ep", "tp", None),
        P("ep", None),
        P("ep", None),
    )
    out_specs = (P("ep", None), P("ep", "tp", None, None))
    return jax.shard_map(shards, mesh=mesh, in_specs=in_specs, out_specs=out_specs, check_vma=False)
```
